256 devices in a mesh: dp: 4 (over x), kv: 32 (over z, y), tp: 2 (over core).
Axes of the slice: x: 4, y: 4, z: 8, core: 2. Of those that a mesh axis runs over, the one named last changes fastest.
Arguments:
- tokens: bfloat16 [32, 4096], P('dp', 'kv'), may hold values from -6 to 6
- token_gain: float32 [4096], P('kv'), may hold values from 0.1 to 1.9
- asker_narrow_matrix: bfloat16 [4096, 1536], P('kv'), may hold values from -0.09375 to 0.09375
- hidden_narrow_matrix: bfloat16 [4096, 1088], P('kv'), may hold values from -0.09375 to 0.09375
- asker_multiplier: float32 [1536], replicated, may hold values from 0.1 to 1.9
- hidden_multiplier: float32 [1024], replicated, may hold values from 0.1 to 1.9
- asker_unspun_matrix: bfloat16 [1536, 64, 128], P(None, ('kv', 'tp')), may hold values from -0.15625 to 0.15625
- asker_spin_matrix: bfloat16 [1536, 64, 64], P(None, ('kv', 'tp')), may hold values from -0.15625 to 0.15625
- lock_widen_matrix: bfloat16 [64, 128, 1024], P(('kv', 'tp')), may hold values from -0.25 to 0.25
- payload_widen_matrix: bfloat16 [64, 1024, 128], P(('kv', 'tp')), may hold values from -0.75 to 0.75
- w_output: bfloat16 [8192, 4096], P(('kv', 'tp')), may hold values from -1.5 to 1.5
- cache_latent: bfloat16 [32, 8192, 1024], P('dp', 'kv'), may hold values from -4 to 4
- cache_rotary: bfloat16 [32, 8192, 64], P('dp', 'kv'), may hold values from -400 to 400
- lengths: int32 [32], P('dp'), may hold values from 4096 to 8191, as said below
Outputs:
- attention_out: float32 [32, 4096], P('dp', ('kv', 'tp'))
- incoming_hidden: float32 [32, 1024], P('dp')
- incoming_spun: float32 [32, 64], P('dp')
The draws below stay inside these ranges and needn't reach their ends.
Inputs may be any that keep to these rules, and one draw needn't show every extreme that they name: `lengths`: each length lies in 4096 to 8191; some sequence has 8191 and some has 4096.
All inputs are finite; a program needn't handle non-finite values.
Results may differ from the reference program's by a relative error of at most 0.015.
Values may be sent and summed in bfloat16 or wider, within the bound.
A program may use at most 64 MiB of HBM per device.

```python
import jax
import jax.numpy as jnp
from jax import lax

MODEL_BREADTH = 4096
ASKER_COUNT = 64
ASK_PACKED = 1536
PACKED_BREADTH = 1024
PLAIN_SPAN = 128
SPIN_SPAN = 64
PAYLOAD_SPAN = 128
BATCH_COUNT = 32
MEMORY_SLOTS = 8192


def draw_cache_latent(key, part):
    shape = (BATCH_COUNT, MEMORY_SLOTS, PACKED_BREADTH)
    values = jnp.clip(jax.random.normal(key, shape, jnp.float32), -4.0, 4.0)
    return values.astype(jnp.bfloat16)


def draw_cache_rotary(key, part):
    shape = (BATCH_COUNT, MEMORY_SLOTS, SPIN_SPAN)
    values = jnp.clip(jax.random.normal(key, shape, jnp.float32), -4.0, 4.0)
    mighty = jax.random.uniform(jax.random.fold_in(key, 7), (BATCH_COUNT, 1, SPIN_SPAN), jnp.float32, -400.0, 400.0)
    chosen_rows = (jnp.arange(BATCH_COUNT) % 4 == 0)[:, None, None]
    slots = jnp.arange(MEMORY_SLOTS)[None, :, None]
    values = jnp.where(chosen_rows & (slots == 3), mighty, values)
    values = jnp.where(chosen_rows & (slots == 5), -mighty, values)
    return values.astype(jnp.bfloat16)


def draw_lengths(key, part):
    values = jax.random.randint(key, (BATCH_COUNT,), MEMORY_SLOTS // 2, MEMORY_SLOTS, dtype=jnp.int32)
    values = values.at[0].set(MEMORY_SLOTS - 1)
    return values.at[BATCH_COUNT - 1].set(MEMORY_SLOTS // 2)


def with_spikes(entries, rng, source, target, parts, factor):
    def block_of(axis_at):
        return (jnp.arange(entries.shape[axis_at]) // (entries.shape[axis_at] // parts)).reshape((-1,) + (1,) * (entries.ndim - 1 - axis_at))

    one_side = jax.random.permutation(rng, parts)[block_of(target)]
    far = (block_of(target) + parts // 2) % parts
    return jnp.where((block_of(source) == one_side) | (block_of(source) == far), factor * entries, entries)


def levels(rng, shape, cuts, smallest, high):
    def one(dim, parts):
        steps = jax.random.uniform(jax.random.fold_in(jax.random.fold_in(rng, 6), dim), (parts,), jnp.float32, smallest / len(cuts), high / len(cuts))
        return jnp.repeat(jnp.exp(steps), shape[dim] // parts).reshape((-1,) + (1,) * (len(shape) - dim - 1))

    level = one(*cuts[0])
    for cut in cuts[1:]:
        level = level * one(*cut)
    return level


def bell_draw(rng, dims, spread, limit, split=(), held_as=jnp.bfloat16):
    drawn = jax.random.normal(rng, dims, jnp.float32) * spread
    if len(split) > 0:
        drawn = levels(rng, dims, split, -0.22, 0.18) * drawn
    return jnp.clip(drawn, min=-limit, max=limit).astype(held_as)


def bell_draw_with(rng, extent, scale, reach, pieces, heavy, held_as=jnp.bfloat16):
    values = scale * jax.random.normal(rng, extent, jnp.float32)
    if pieces:
        values = values * levels(rng, extent, pieces, -0.22, 0.18)
    return jnp.clip(with_spikes(values, jax.random.fold_in(rng, 3), *heavy), -reach, reach).astype(held_as)


def setup_inputs(seed: int = 0) -> dict:
    streams_of = jax.random.split(jax.random.key(seed), 15)
    tokens = bell_draw(streams_of[0], (BATCH_COUNT, MODEL_BREADTH), 1.0, 6.0, ((0, 4), (1, 32)))
    token_gain = jnp.clip(1.0 + 0.18 * jax.random.normal(streams_of[1], (MODEL_BREADTH,), jnp.float32), 0.1, 1.9)
    asker_narrow_matrix = bell_draw(streams_of[2], (MODEL_BREADTH, ASK_PACKED), MODEL_BREADTH ** -0.5, 0.09375, ((0, 32),))
    hidden_narrow_matrix = bell_draw(streams_of[3], (MODEL_BREADTH, PACKED_BREADTH + SPIN_SPAN), MODEL_BREADTH ** -0.5, 0.09375, ((0, 32),))
    asker_multiplier = jnp.clip(1.0 + 0.18 * jax.random.normal(streams_of[4], (ASK_PACKED,), jnp.float32), 0.1, 1.9)
    hidden_multiplier = jnp.clip(1.0 + 0.18 * jax.random.normal(streams_of[5], (PACKED_BREADTH,), jnp.float32), 0.1, 1.9)
    asker_unspun_matrix = bell_draw(streams_of[6], (ASK_PACKED, ASKER_COUNT, PLAIN_SPAN), ASK_PACKED ** -0.5, 0.15625, ((1, 64),))
    asker_spin_matrix = bell_draw(streams_of[7], (ASK_PACKED, ASKER_COUNT, SPIN_SPAN), ASK_PACKED ** -0.5, 0.15625, ((1, 64),))
    lock_widen_matrix = bell_draw(streams_of[8], (ASKER_COUNT, PLAIN_SPAN, PACKED_BREADTH), (4 * PLAIN_SPAN) ** -0.5, 0.25, ((0, 64),))
    payload_widen_matrix = bell_draw(streams_of[9], (ASKER_COUNT, PACKED_BREADTH, PAYLOAD_SPAN), (PACKED_BREADTH // 16) ** -0.5, 0.75, ((0, 64),))
    w_output = bell_draw_with(streams_of[10], (ASKER_COUNT * PAYLOAD_SPAN, MODEL_BREADTH), (ASKER_COUNT * PAYLOAD_SPAN // 64) ** -0.5, 1.5, ((0, 64),), (0, 1, 64, 4.0))
    cache_latent = draw_cache_latent(jax.random.fold_in(streams_of[14], 71), 0)
    cache_rotary = draw_cache_rotary(jax.random.fold_in(streams_of[14], 71), 0)
    lengths = draw_lengths(jax.random.fold_in(streams_of[14], 71), 0)
    return dict(tokens=tokens, token_gain=token_gain, asker_narrow_matrix=asker_narrow_matrix, hidden_narrow_matrix=hidden_narrow_matrix, asker_multiplier=asker_multiplier, hidden_multiplier=hidden_multiplier, asker_unspun_matrix=asker_unspun_matrix, asker_spin_matrix=asker_spin_matrix, lock_widen_matrix=lock_widen_matrix, payload_widen_matrix=payload_widen_matrix, w_output=w_output, cache_latent=cache_latent, cache_rotary=cache_rotary, lengths=lengths)


EPS = 1e-06
THETA = 10000.0

def magnitude_divisor(values, gain):
    mean_square = lax.optimization_barrier(jnp.mean(values * values, axis=-1, keepdims=True))
    return values * lax.rsqrt(mean_square + EPS) * gain

def spinning(values, position):
    half_width = values.shape[-1] // 2
    exponent = jnp.arange(half_width, dtype=jnp.float32) * (2.0 / values.shape[-1])
    frequency = THETA ** (-exponent)
    angles = position.astype(jnp.float32)[:, None] * frequency[None, :]
    angles = angles.reshape((angles.shape[0],) + (1,) * (values.ndim - 2) + (half_width,))
    cosine = jnp.cos(angles)
    sine_table = jnp.sin(angles)
    former = values[..., :half_width]
    latter = values[..., half_width:]
    return jnp.concatenate([former * cosine - latter * sine_table, former * sine_table + latter * cosine], axis=-1)

def reference(tokens, token_gain, asker_narrow_matrix, hidden_narrow_matrix, asker_multiplier, hidden_multiplier, asker_unspun_matrix, asker_spin_matrix, lock_widen_matrix, payload_widen_matrix, w_output, cache_latent, cache_rotary, lengths):
    tokens_wide = tokens.astype(jnp.float32)
    squares = lax.optimization_barrier(jnp.sum(tokens_wide * tokens_wide, axis=1, keepdims=True))
    row_scale = lax.rsqrt(squares / MODEL_BREADTH + EPS)
    scaled = (tokens_wide * token_gain).astype(jnp.bfloat16)
    query_down = jnp.dot(scaled, asker_narrow_matrix, preferred_element_type=jnp.float32) * row_scale
    hidden_squeeze = jnp.dot(scaled, hidden_narrow_matrix, preferred_element_type=jnp.float32) * row_scale
    squeezed = magnitude_divisor(query_down, asker_multiplier).astype(jnp.bfloat16)
    incoming_hidden = magnitude_divisor(hidden_squeeze[:, :PACKED_BREADTH], hidden_multiplier)
    incoming_spun = spinning(hidden_squeeze[:, PACKED_BREADTH:], lengths)
    fresh_hidden = incoming_hidden.astype(jnp.bfloat16)
    fresh_spun = incoming_spun.astype(jnp.bfloat16)
    asker_unspun = jnp.dot(squeezed, asker_unspun_matrix.reshape(ASK_PACKED, ASKER_COUNT * PLAIN_SPAN), preferred_element_type=jnp.float32)
    asker_unspun = asker_unspun.reshape(BATCH_COUNT, ASKER_COUNT, PLAIN_SPAN).astype(jnp.bfloat16)
    query_latent = jnp.einsum('bhd,hdc->bhc', asker_unspun.astype(jnp.float32), lock_widen_matrix.astype(jnp.float32)).astype(jnp.bfloat16)
    asker_spun = jnp.dot(squeezed, asker_spin_matrix.reshape(ASK_PACKED, ASKER_COUNT * SPIN_SPAN), preferred_element_type=jnp.float32)
    asker_spun = spinning(asker_spun.reshape(BATCH_COUNT, ASKER_COUNT, SPIN_SPAN), lengths).astype(jnp.bfloat16)
    positions = jnp.arange(MEMORY_SLOTS, dtype=jnp.int32)
    score_scale = (PLAIN_SPAN + SPIN_SPAN) ** (-0.5)

    def attend(per_sequence):
        one_latent, one_turned, keys_latent, keys_turned, fresh_latent, fresh_turned, length = per_sequence
        fresh_slot = positions == length
        keys_latent = jnp.where(fresh_slot[:, None], fresh_latent[None, :], keys_latent).astype(jnp.float32)
        keys_turned = jnp.where(fresh_slot[:, None], fresh_turned[None, :], keys_turned).astype(jnp.float32)
        scores = jnp.dot(one_latent.astype(jnp.float32), keys_latent.T) + jnp.dot(one_turned.astype(jnp.float32), keys_turned.T)
        scores = scores * score_scale
        visible = (positions <= length)[None, :]
        scores = jnp.where(visible, scores, -1e+30)
        highest = lax.optimization_barrier(jnp.max(scores, axis=1, keepdims=True))
        weights = jnp.where(visible, jnp.exp(scores - highest), 0.0)
        denominator = lax.optimization_barrier(jnp.sum(weights, axis=1, keepdims=True))
        rounded = lax.optimization_barrier(weights.astype(jnp.bfloat16)).astype(jnp.float32)
        mixture = jnp.dot(rounded, keys_latent)
        return (mixture / denominator).astype(jnp.bfloat16)
    attended = lax.map(attend, (query_latent, asker_spun, cache_latent, cache_rotary, fresh_hidden, fresh_spun, lengths))
    head_values = jnp.einsum('bhc,hcv->bhv', attended.astype(jnp.float32), payload_widen_matrix.astype(jnp.float32)).astype(jnp.bfloat16)
    output = jnp.dot(head_values.reshape(BATCH_COUNT, ASKER_COUNT * PAYLOAD_SPAN), w_output, preferred_element_type=jnp.float32)
    return (output, incoming_hidden, incoming_spun)
```

```python
import functools

import jax
import jax.numpy as jnp
from jax import lax
from jax.experimental import pallas as pl
from jax.experimental.pallas import tpu as pltpu
from jax.sharding import PartitionSpec as P

MODEL_BREADTH = 4096
EPS = 1e-06
THETA = 10000.0
RING = 4
MESH = pl.DeviceIdType.MESH
F32 = jnp.float32
BF16 = jnp.bfloat16


def across(a, b):
    return lax.dot_general(a, b, (((1,), (1,)), ((), ())), preferred_element_type=F32)


def plain(a, b):
    return jnp.dot(a, b, preferred_element_type=F32)


def kernel(
    depth,
    tokens_hbm,
    gain_hbm,
    ask_hbm,
    hid_hbm,
    ask_gain_hbm,
    hid_gain_hbm,
    unspun_hbm,
    spin_hbm,
    lock_hbm,
    payload_hbm,
    out_hbm,
    latent_hbm,
    rotary_hbm,
    frequency_hbm,
    lengths,
    attention_out,
    hidden_out,
    spun_out,
    tokens,
    gain,
    ask,
    hid,
    ask_gain,
    hid_gain,
    unspun,
    spin,
    lock,
    payload,
    w_out,
    latent,
    rotary,
    frequency,
    part_send,
    part_recv,
    mid_recv,
    full,
    queries,
    scores,
    spread,
    stat_send,
    stat_recv,
    mix_send,
    mix_recv,
    stat2_send,
    stat2_recv,
    mix2_send,
    mix2_recv,
    out_send,
    out_recv,
    out2_send,
    out2_recv,
    local_sem,
    part_sems,
    mid_sems,
    full_sems,
    qz_sems,
    qy_sems,
    stat_sems,
    mix_sems,
    stat2_sems,
    mix2_sems,
    out_sems,
    out2_sems,
):
    kv = lax.axis_index("kv")
    tp = lax.axis_index("tp")
    z, y = kv // RING, kv % RING
    span = 256

    def at(zz, yy, cc=None):
        where = {"kv": zz * RING + yy}
        if cc is not None:
            where["tp"] = cc
        return where

    def zp(d):
        return (z + d) % depth

    def zm(d):
        return (z + depth - d) % depth

    def yp(d):
        return (y + d) % RING

    def ym(d):
        return (y + RING - d) % RING

    pending = []

    def send(src, dst, sems, index, device):
        copy = pltpu.make_async_remote_copy(
            src_ref=src,
            dst_ref=dst,
            send_sem=sems.at[(0, *index)],
            recv_sem=sems.at[(1, *index)],
            device_id=device,
            device_id_type=MESH,
        )
        copy.start()
        pending.append(copy)
        return copy

    barrier = pltpu.get_barrier_semaphore()
    greeted = 0
    for d in range(1, depth):
        pl.semaphore_signal(barrier, inc=1, device_id=at(zp(d), y), device_id_type=MESH)
        greeted += 1
    for d in range(RING):
        for c in range(2):
            if d or c:
                pl.semaphore_signal(
                    barrier, inc=1, device_id=at(z, yp(d), (tp + c) % 2), device_id_type=MESH
                )
                greeted += 1

    loads = {}
    for k, (name, src, dst) in enumerate(
        (
            ("tokens", tokens_hbm, tokens),
            ("gain", gain_hbm, gain),
            ("ask", ask_hbm, ask),
            ("hid", hid_hbm, hid),
            ("ask_gain", ask_gain_hbm, ask_gain),
            ("hid_gain", hid_gain_hbm, hid_gain),
            ("frequency", frequency_hbm, frequency),
            ("unspun", unspun_hbm, unspun),
            ("spin", spin_hbm, spin),
            ("lock", lock_hbm, lock),
            ("rotary", rotary_hbm, rotary),
            ("latent", latent_hbm, latent),
            ("payload", payload_hbm, payload),
            ("w_out", out_hbm, w_out),
        )
    ):
        loads[name] = pltpu.make_async_copy(src, dst, local_sem.at[k])
        loads[name].start()

    for name in ("tokens", "gain", "ask", "hid"):
        loads[name].wait()
    wide = tokens[...].astype(F32)
    squares = jnp.sum(wide * wide, axis=1, keepdims=True)
    scaled = (wide * gain[...]).astype(BF16)
    query_part = plain(scaled, ask[...])
    latent_part = across(scaled, hid[...])
    tiles = [query_part[:, 128 * t : 128 * t + 128] for t in range(12)]
    tiles += [latent_part[:, 128 * t : 128 * t + 128] for t in range(8)]
    tiles += [
        jnp.concatenate([latent_part[:, 1024:1088], jnp.broadcast_to(squares, (8, 64))], axis=1)
    ]
    tiles += [jnp.zeros((8, 128), F32)] * 3
    for t, tile in enumerate(tiles):
        part_send[t // 3, t % 3] = tile
    part_recv[pl.ds(z, 1)] = part_send[pl.ds(z, 1)]

    pl.semaphore_wait(barrier, greeted)
    copies = [
        send(part_send.at[zp(d)], part_recv.at[z], part_sems, (d,), at(zp(d), y))
        for d in range(1, depth)
    ]

    for name in ("ask_gain", "hid_gain", "frequency"):
        loads[name].wait()
    row8 = lax.broadcasted_iota(jnp.int32, (8, 128), 0)
    length_rows = jnp.zeros((8, 128), jnp.int32)
    for s in range(8):
        length_rows = jnp.where(row8 == s, lengths[s], length_rows)
    angles = length_rows.astype(F32) * frequency[...]
    lane8 = lax.broadcasted_iota(jnp.int32, (8, 128), 1)
    cosine = jnp.cos(angles)
    sine = jnp.where(lane8 % 64 < 32, -jnp.sin(angles), jnp.sin(angles))

    def spinning(v):
        twice = jnp.concatenate([v, v], axis=1)
        return twice * cosine + pltpu.roll(twice, 32, 1) * sine

    for copy in copies:
        copy.wait_recv()
    total = part_recv[0]
    for j in range(1, depth):
        total = total + part_recv[j]
    mid_recv[pl.ds(y, 1)] = total[None]
    copies = [
        send(mid_recv.at[y], mid_recv.at[y], mid_sems, (d,), at(z, yp(d))) for d in range(1, RING)
    ]
    for copy in copies:
        copy.wait_recv()
    total = mid_recv[0]
    for j in range(1, RING):
        total = total + mid_recv[j]
    full[pl.ds(z, 1)] = total[None]
    copies = [
        send(full.at[z], full.at[z], full_sems, (d,), at(zp(d), y)) for d in range(1, depth)
    ]
    for name in ("unspun", "spin", "lock"):
        loads[name].wait()
    for copy in copies:
        copy.wait_recv()

    last = full[6, 2]
    row_scale = lax.rsqrt(last[:, 64:65] / MODEL_BREADTH + EPS)
    query_down = jnp.concatenate([full[t // 3, t % 3] for t in range(12)], axis=1) * row_scale
    mean_square = jnp.mean(query_down * query_down, axis=1, keepdims=True)
    squeezed = (query_down * lax.rsqrt(mean_square + EPS) * ask_gain[...]).astype(BF16)
    nope = plain(squeezed, unspun[...]).astype(BF16)
    turned = spinning(across(squeezed, spin[...])).astype(BF16)
    queries[0, 0, :, 1024:1152] = turned
    queries[0, 0, :, 0:1024] = plain(nope, lock[...]).astype(BF16)

    order = sorted(range(1, depth), key=lambda d: min(d, depth - d))
    from_z = {
        d: send(queries.at[0, 0], queries.at[0, d], qz_sems, (d,), at(zp(d), y)) for d in order
    }
    from_y = [
        send(queries.at[0, 0], queries.at[e, 0], qy_sems, (e, 0), at(z, yp(e)))
        for e in range(1, RING)
    ]

    hidden_down = jnp.concatenate([full[t // 3, t % 3] for t in range(12, 20)], axis=1) * row_scale
    mean_square = jnp.mean(hidden_down * hidden_down, axis=1, keepdims=True)
    incoming_hidden = hidden_down * lax.rsqrt(mean_square + EPS) * hid_gain[...]
    incoming_spun = spinning(last[:, 0:64] * row_scale)[:, 0:64]
    hidden_out[...] = incoming_hidden
    spun_out[...] = incoming_spun

    def forward(d):
        from_z[d].wait_recv()
        for e in range(1, RING):
            from_y.append(
                send(queries.at[0, d], queries.at[e, d], qy_sems, (e, d), at(z, yp(e)))
            )

    loads["latent"].wait()
    loads["rotary"].wait()
    eye = (
        lax.broadcasted_iota(jnp.int32, (64, 64), 0) == lax.broadcasted_iota(jnp.int32, (64, 64), 1)
    ).astype(BF16)
    spun_columns = across(eye, incoming_spun.astype(BF16))
    position_row = kv * span + lax.broadcasted_iota(jnp.int32, (64, span), 1)
    position_column = kv * span + lax.broadcasted_iota(jnp.int32, (span, 1024), 0)
    for s in range(8):
        rotary[s] = jnp.where(
            position_row == lengths[s], spun_columns[:, s : s + 1], rotary[s].astype(F32)
        ).astype(BF16)
        latent[span * s : span * s + span] = jnp.where(
            position_column == lengths[s],
            incoming_hidden[s : s + 1],
            latent[span * s : span * s + span].astype(F32),
        ).astype(BF16)
        if s < depth - 1:
            forward(order[s])
    for copy in from_y:
        copy.wait_recv()

    rows = 8 * RING * depth
    everything = queries[...].reshape(rows, 1152)
    sequence = lax.broadcasted_iota(jnp.int32, (rows, span), 0) % 8

    @pl.loop(0, 8)
    def _(s):
        block = latent[pl.ds(pl.multiple_of(s * span, span), span), :]
        found = across(everything[:, 0:1024], block) + plain(everything[:, 1024:1088], rotary[s])
        scores[...] = jnp.where(sequence == s, found, scores[...])

    grouped = (RING * depth, 8, span)
    position = kv * span + lax.broadcasted_iota(jnp.int32, grouped, 2)
    lengths_wide = jnp.concatenate([length_rows, length_rows], axis=1)
    visible = position <= lengths_wide[None]
    score = jnp.where(visible, scores[...].reshape(grouped) * (192.0**-0.5), -1e30)
    highest = jnp.max(score, axis=2, keepdims=True)
    high = highest.astype(BF16).astype(F32)
    low = (highest - high).astype(BF16).astype(F32)
    highest = high + low
    weight = jnp.where(visible, jnp.exp(score - highest), 0.0)
    denominator = jnp.sum(weight, axis=2, keepdims=True)

    def statistics(m_high, m_low, total):
        t_high = total.astype(BF16).astype(F32)
        lane = lax.broadcasted_iota(jnp.int32, (*total.shape[:2], 128), 2)
        return jnp.where(
            lane == 0,
            m_high,
            jnp.where(lane == 1, m_low, jnp.where(lane == 2, t_high, total - t_high)),
        ).astype(BF16)

    stat_send[...] = statistics(high, low, denominator).reshape(RING, depth, 8, 128)
    stat_copies = [
        send(stat_send.at[e], stat_recv.at[e], stat_sems, (e,), at(z, ym(e)))
        for e in range(1, RING)
    ]
    flat = weight.reshape(rows, span)
    for s in range(8):
        spread[:, span * s : span * s + span] = jnp.where(sequence == s, flat, 0.0).astype(BF16)

    mix_copies = []
    for n in range(4):
        found = plain(spread[...], latent[:, 256 * n : 256 * n + 256])
        mix_send[n] = found.astype(BF16).reshape(RING, depth, 8, 256)
        mix_copies.append(
            [
                send(mix_send.at[n, e], mix_recv.at[n, e], mix_sems, (n, e), at(z, ym(e)))
                for e in range(1, RING)
            ]
        )

    def combine(stats):
        tops = [b[:, :, 0:1] + b[:, :, 1:2] for b in stats]
        sums = [b[:, :, 2:3] + b[:, :, 3:4] for b in stats]
        top = functools.reduce(jnp.maximum, tops)
        factors = [jnp.exp(t - top) for t in tops]
        return top, sum(f * v for f, v in zip(factors, sums)), factors

    for copy in stat_copies:
        copy.wait_recv()
    top, total, factors = combine(
        [stat_send[0].astype(F32)] + [stat_recv[e].astype(F32) for e in range(1, RING)]
    )
    high = top.astype(BF16).astype(F32)
    stat2_send[...] = statistics(high, top - high, total)
    stat2_copies = [
        send(stat2_send.at[d], stat2_recv.at[d], stat2_sems, (d,), at(zm(d), y))
        for d in range(1, depth)
    ]
    mix2_copies = []
    for n in range(4):
        for copy in mix_copies[n]:
            copy.wait_recv()
        found = factors[0] * mix_send[n, 0].astype(F32)
        for e in range(1, RING):
            found = found + factors[e] * mix_recv[n, e].astype(F32)
        mix2_send[n] = found.astype(BF16)
        mix2_copies.append(
            [
                send(mix2_send.at[n, d], mix2_recv.at[n, d], mix2_sems, (n, d), at(zm(d), y))
                for d in range(1, depth)
            ]
        )

    for copy in stat2_copies:
        copy.wait_recv()
    _, total, factors = combine(
        [stat2_send[0:1].astype(F32)] + [stat2_recv[d : d + 1].astype(F32) for d in range(1, depth)]
    )
    factors = [f[0] for f in factors]
    attended = []
    for n in range(4):
        for copy in mix2_copies[n]:
            copy.wait_recv()
        found = factors[0] * mix2_send[n, 0].astype(F32)
        for d in range(1, depth):
            found = found + factors[d] * mix2_recv[n, d].astype(F32)
        attended.append((found / total[0]).astype(BF16))

    loads["payload"].wait()
    loads["w_out"].wait()
    values = plain(jnp.concatenate(attended, axis=1), payload[...]).astype(BF16)
    projected = plain(values, w_out[...])
    first = lane8 < 64
    for i in range(depth // 2):
        for j in range(RING):
            a = 128 * (2 * i * RING + j)
            b = 128 * ((2 * i + 1) * RING + j)
            one, two = projected[:, a : a + 128], projected[:, b : b + 128]
            out_send[j, 0, i] = jnp.where(first, one, pltpu.roll(two, 64, 1)).astype(BF16)
            out_send[j, 1, i] = jnp.where(first, pltpu.roll(one, 64, 1), two).astype(BF16)
    copies = []
    for e in range(RING):
        for c in range(2):
            if e or c:
                core = (tp + c) % 2
                copies.append(
                    send(
                        out_send.at[yp(e), core],
                        out_recv.at[2 * e + c],
                        out_sems,
                        (2 * e + c,),
                        at(z, yp(e), core),
                    )
                )
    found = out_send[y, tp].astype(F32)
    for copy in copies:
        copy.wait_recv()
    for k in range(1, 2 * RING):
        found = found + out_recv[k].astype(F32)
    out2_send[...] = found.astype(BF16)
    copies = [
        send(out2_send.at[zp(d) // 2], out2_recv.at[d], out2_sems, (d,), at(zp(d), y))
        for d in range(1, depth)
    ]
    found = out2_send[z // 2].astype(F32)
    for copy in copies:
        copy.wait_recv()
    for d in range(1, depth):
        found = found + out2_recv[d].astype(F32)
    attention_out[...] = jnp.where(z % 2 == 0, found[:, 0:64], found[:, 64:128])
    for copy in pending:
        copy.wait_send()


def local(
    depth,
    tokens,
    token_gain,
    asker_narrow_matrix,
    hidden_narrow_matrix,
    asker_multiplier,
    hidden_multiplier,
    asker_unspun_matrix,
    asker_spin_matrix,
    lock_widen_matrix,
    payload_widen_matrix,
    w_output,
    cache_latent,
    cache_rotary,
    lengths,
):
    exponent = (jnp.arange(128) % 32).astype(F32) * (2.0 / 64)
    frequency = (THETA ** (-exponent))[None]
    operands = (
        tokens,
        token_gain.reshape(1, 128),
        asker_narrow_matrix,
        hidden_narrow_matrix.T,
        asker_multiplier.reshape(1, 1536),
        hidden_multiplier.reshape(1, 1024),
        asker_unspun_matrix.reshape(1536, 128),
        asker_spin_matrix.reshape(1536, 64).T,
        lock_widen_matrix.reshape(128, 1024),
        payload_widen_matrix.reshape(1024, 128),
        w_output,
        cache_latent.reshape(2048, 1024),
        jnp.swapaxes(cache_rotary, 1, 2),
        frequency,
    )
    hbm = pl.BlockSpec(memory_space=pl.ANY)
    vmem = pl.BlockSpec(memory_space=pltpu.VMEM)
    dma = pltpu.SemaphoreType.DMA
    return pl.pallas_call(
        functools.partial(kernel, depth),
        out_shape=(
            jax.ShapeDtypeStruct((8, 64), F32),
            jax.ShapeDtypeStruct((8, 1024), F32),
            jax.ShapeDtypeStruct((8, 64), F32),
        ),
        in_specs=[hbm] * len(operands) + [pl.BlockSpec(memory_space=pltpu.SMEM)],
        out_specs=(vmem, vmem, vmem),
        scratch_shapes=[pltpu.VMEM(a.shape, a.dtype) for a in operands]
        + [
            pltpu.VMEM((depth, 3, 8, 128), F32),
            pltpu.VMEM((depth, 3, 8, 128), F32),
            pltpu.VMEM((RING, 3, 8, 128), F32),
            pltpu.VMEM((depth, 3, 8, 128), F32),
            pltpu.VMEM((RING, depth, 8, 1152), BF16),
            pltpu.VMEM((8 * RING * depth, 256), F32),
            pltpu.VMEM((8 * RING * depth, 2048), BF16),
            pltpu.VMEM((RING, depth, 8, 128), BF16),
            pltpu.VMEM((RING, depth, 8, 128), BF16),
            pltpu.VMEM((4, RING, depth, 8, 256), BF16),
            pltpu.VMEM((4, RING, depth, 8, 256), BF16),
            pltpu.VMEM((depth, 8, 128), BF16),
            pltpu.VMEM((depth, 8, 128), BF16),
            pltpu.VMEM((4, depth, 8, 256), BF16),
            pltpu.VMEM((4, depth, 8, 256), BF16),
            pltpu.VMEM((RING, 2, depth // 2, 8, 128), BF16),
            pltpu.VMEM((2 * RING, depth // 2, 8, 128), BF16),
            pltpu.VMEM((depth // 2, 8, 128), BF16),
            pltpu.VMEM((depth, 8, 128), BF16),
            dma((len(operands),)),
            dma((2, depth)),
            dma((2, RING)),
            dma((2, depth)),
            dma((2, depth)),
            dma((2, RING, depth)),
            dma((2, RING)),
            dma((2, 4, RING)),
            dma((2, depth)),
            dma((2, 4, depth)),
            dma((2, 2 * RING)),
            dma((2, depth)),
        ],
        compiler_params=pltpu.CompilerParams(collective_id=0, has_side_effects=True),
    )(*operands, lengths)


def solution(mesh):
    return jax.shard_map(
        functools.partial(local, mesh.shape["kv"] // RING),
        mesh=mesh,
        in_specs=(
            P("dp", "kv"),
            P("kv"),
            P("kv", None),
            P("kv", None),
            P(),
            P(),
            P(None, ("kv", "tp"), None),
            P(None, ("kv", "tp"), None),
            P(("kv", "tp"), None, None),
            P(("kv", "tp"), None, None),
            P(("kv", "tp"), None),
            P("dp", "kv", None),
            P("dp", "kv", None),
            P("dp"),
        ),
        out_specs=(P("dp", ("kv", "tp")), P("dp", None), P("dp", None)),
        check_vma=False,
    )
```

```python
import functools

import jax
import jax.numpy as jnp
from jax import lax
from jax.experimental import pallas as pl
from jax.experimental.pallas import tpu as pltpu
from jax.sharding import PartitionSpec as P

MODEL_BREADTH = 4096
EPS = 1e-06
THETA = 10000.0
RING = 4
MESH = pl.DeviceIdType.MESH
PART, MID, FULL, ASK_Y, ASK_Z, MIX, MIX2, OUT, OUT2, PHASES = 0, 1, 2, 3, 8, 16, 24, 25, 26, 27
F32 = jnp.float32
BF16 = jnp.bfloat16


def across(a, b):
    return lax.dot_general(a, b, (((1,), (1,)), ((), ())), preferred_element_type=F32)


def plain(a, b):
    return jnp.dot(a, b, preferred_element_type=F32)


def kernel(
    depth,
    tokens_hbm,
    gain_hbm,
    ask_hbm,
    hid_hbm,
    ask_gain_hbm,
    hid_gain_hbm,
    unspun_hbm,
    spin_hbm,
    lock_hbm,
    payload_hbm,
    out_hbm,
    latent_hbm,
    rotary_hbm,
    lengths_hbm,
    attention_out,
    hidden_out,
    spun_out,
    tokens,
    gain,
    ask,
    hid,
    ask_gain,
    hid_gain,
    unspun,
    spin,
    lock,
    payload,
    w_out,
    latent,
    rotary,
    part_send,
    part_recv,
    mid_recv,
    full,
    queries,
    sorted_queries,
    mix_own,
    mix_send,
    mix_recv,
    mix2_send,
    mix2_recv,
    out_send,
    out_recv,
    out2_send,
    out2_recv,
    local_sem,
    sent_sems,
    come_sems,
    lengths,
):
    kv = lax.axis_index("kv")
    tp = lax.axis_index("tp")
    z, y = kv // RING, kv % RING
    span = 256
    near_first = sorted(range(1, depth), key=lambda d: min(d, depth - d))
    order = (1, 3, 2)

    def at(zz, yy, cc=None):
        where = {"kv": zz * RING + yy}
        if cc is not None:
            where["tp"] = cc
        return where

    def zp(d):
        return (z + d) % depth

    def zm(d):
        return (z + depth - d) % depth

    def yp(d):
        return (y + d) % RING

    def ym(d):
        return (y + RING - d) % RING

    def describe(src, dst, phase, arrival, device):
        return pltpu.make_async_remote_copy(
            src_ref=src,
            dst_ref=dst,
            send_sem=sent_sems.at[phase],
            recv_sem=come_sems.at[arrival],
            device_id=device,
            device_id_type=MESH,
        )

    def send(src, dst, phase, arrival, device):
        describe(src, dst, phase, arrival, device).start()

    def arrived(ref, arrival):
        describe(ref, ref, 0, arrival, at(z, y)).wait_recv()

    plane = [(e, c) for e in (*order, 0) for c in range(2) if e or c]

    barrier = pltpu.get_barrier_semaphore()
    for d in near_first:
        pl.semaphore_signal(barrier, inc=1, device_id=at(zp(d), y), device_id_type=MESH)
    for e, c in plane:
        pl.semaphore_signal(
            barrier, inc=1, device_id=at(z, yp(e), (tp + c) % 2), device_id_type=MESH
        )
    greeted = len(near_first) + len(plane)

    loads = {}

    def load(**pairs):
        for name, (src, dst) in pairs.items():
            loads[name] = pltpu.make_async_copy(src, dst, local_sem.at[len(started)])
            started.append(name)
            loads[name].start()

    started = []
    load(
        tokens=(tokens_hbm, tokens),
        gain=(gain_hbm, gain),
        ask=(ask_hbm, ask),
        hid=(hid_hbm, hid),
    )

    for name in ("tokens", "gain", "ask", "hid"):
        loads.pop(name).wait()
    load(
        lengths=(lengths_hbm, lengths),
        ask_gain=(ask_gain_hbm, ask_gain),
        hid_gain=(hid_gain_hbm, hid_gain),
        unspun=(unspun_hbm, unspun),
        spin=(spin_hbm, spin),
        lock=(lock_hbm, lock),
        rotary=(rotary_hbm, rotary),
        latent=(latent_hbm, latent),
        payload=(payload_hbm, payload),
        w_out=(out_hbm, w_out),
    )
    wide = tokens[...].astype(F32)
    squares = jnp.sum(wide * wide, axis=1, keepdims=True)
    scaled = (wide * gain[...]).astype(BF16)
    query_part = plain(scaled, ask[...])
    latent_part = across(scaled, hid[...])
    tiles = [query_part[:, 128 * t : 128 * t + 128] for t in range(12)]
    tiles += [latent_part[:, 128 * t : 128 * t + 128] for t in range(8)]
    tiles += [
        jnp.concatenate([latent_part[:, 1024:1088], jnp.broadcast_to(squares, (8, 64))], axis=1)
    ]
    tiles += [jnp.zeros((8, 128), F32)] * 3
    for t, tile in enumerate(tiles):
        part_send[t // 6, t // 3 % 2, t % 3] = tile

    pl.semaphore_wait(barrier, greeted)
    for e in order:
        send(part_send.at[yp(e), tp], part_recv.at[e - 1], PART, PART, at(z, yp(e)))

    loads.pop("lengths").wait()
    row8 = lax.broadcasted_iota(jnp.int32, (8, 128), 0)
    lane8 = lax.broadcasted_iota(jnp.int32, (8, 128), 1)
    length_rows = jnp.zeros((8, 128), jnp.int32)
    frequency = jnp.zeros((8, 128), F32)
    for s in range(8):
        length_rows = jnp.where(row8 == s, lengths[s], length_rows)
    for i in range(32):
        frequency = jnp.where(lane8 % 32 == i, float(THETA ** (-i / 32)), frequency)
    angles = length_rows.astype(F32) * frequency
    cosine = jnp.cos(angles)
    sine = jnp.where(lane8 % 64 < 32, -jnp.sin(angles), jnp.sin(angles))

    def spinning(v):
        twice = jnp.concatenate([v, v], axis=1)
        return twice * cosine + pltpu.roll(twice, 32, 1) * sine

    total = part_send[y, tp]
    arrived(part_recv, PART)
    for e in range(RING - 1):
        total = total + part_recv[e]
    mid_recv[pl.ds(z, 1)] = total[None]
    for d in near_first:
        send(mid_recv.at[z], mid_recv.at[z], MID, MID, at(zp(d), y))
    arrived(mid_recv.at[1:depth], MID)
    total = mid_recv[0]
    for j in range(1, depth):
        total = total + mid_recv[j]
    full[pl.ds(2 * y + tp, 1)] = total[None]
    mine = full.at[2 * y + tp]
    for e, c in plane:
        send(mine, mine, FULL, FULL, at(z, yp(e), (tp + c) % 2))
    for name in ("unspun", "spin", "lock", "ask_gain", "hid_gain"):
        loads.pop(name).wait()
    arrived(full.at[1 : 2 * RING], FULL)

    last = full[6, 2]
    row_scale = lax.rsqrt(last[:, 64:65] / MODEL_BREADTH + EPS)
    query_down = jnp.concatenate([full[t // 3, t % 3] for t in range(12)], axis=1) * row_scale
    mean_square = jnp.mean(query_down * query_down, axis=1, keepdims=True)
    ask_gains = jnp.concatenate([ask_gain[t : t + 1] for t in range(12)], axis=1)
    squeezed = (query_down * lax.rsqrt(mean_square + EPS) * ask_gains).astype(BF16)
    nope = plain(squeezed, unspun[...]).astype(BF16)
    turned = spinning(across(squeezed, spin[...])).astype(BF16)
    queries[0, 0, :, 1024:1152] = turned
    queries[0, 0, :, 0:1024] = plain(nope, lock[...]).astype(BF16)

    def to_plane(d):
        for e in order:
            send(queries.at[0, d], queries.at[e, d], ASK_Y, ASK_Y + e, at(z, yp(e)))

    for d in near_first:
        send(queries.at[0, 0], queries.at[0, d], ASK_Z, ASK_Z + d, at(zp(d), y))
    to_plane(0)

    hidden_down = jnp.concatenate([full[t // 3, t % 3] for t in range(12, 20)], axis=1) * row_scale
    mean_square = jnp.mean(hidden_down * hidden_down, axis=1, keepdims=True)
    incoming_hidden = hidden_down * lax.rsqrt(mean_square + EPS) * hid_gain[...]
    incoming_spun = spinning(last[:, 0:64] * row_scale)[:, 0:64]
    hidden_out[...] = incoming_hidden
    spun_out[...] = incoming_spun

    loads.pop("latent").wait()
    loads.pop("rotary").wait()
    eye = (
        lax.broadcasted_iota(jnp.int32, (64, 64), 0) == lax.broadcasted_iota(jnp.int32, (64, 64), 1)
    ).astype(BF16)
    spun_columns = across(eye, incoming_spun.astype(BF16))
    position_row = kv * span + lax.broadcasted_iota(jnp.int32, (64, span), 1)
    position_column = kv * span + lax.broadcasted_iota(jnp.int32, (span, 1024), 0)
    for s in range(8):
        rotary[s] = jnp.where(
            position_row == lengths[s], spun_columns[:, s : s + 1], rotary[s].astype(F32)
        ).astype(BF16)
        latent[span * s : span * s + span] = jnp.where(
            position_column == lengths[s],
            incoming_hidden[s : s + 1],
            latent[span * s : span * s + span].astype(F32),
        ).astype(BF16)
        if s < depth - 1:
            d = near_first[s]
            arrived(queries.at[0, d], ASK_Z + d)
            to_plane(d)

    group = 8 * depth
    come = lax.broadcasted_iota(jnp.int32, (group, group), 1)
    went = lax.broadcasted_iota(jnp.int32, (group, group), 0)
    shuffle = (come == went % depth * 8 + went // depth).astype(BF16)

    def sort_rows(e):
        found = plain(shuffle, queries[e].reshape(group, 1152)).astype(BF16)
        sorted_queries[:, e] = found.reshape(8, depth, 1152)

    sort_rows(0)
    for e in order:
        arrived(queries.at[e], ASK_Y + e)
        sort_rows(e)

    heads = RING * depth
    position = kv * span + lax.broadcasted_iota(jnp.int32, (heads, span), 1)
    lane = lax.broadcasted_iota(jnp.int32, (heads, 128), 1)

    def halves(value):
        high = value.astype(BF16).astype(F32)
        return high, (value - high).astype(BF16).astype(F32)

    def score(s):
        block = latent[span * s : span * s + span]
        asked = sorted_queries[s].reshape(heads, 1152)
        return across(asked[:, 0:1024], block) + plain(asked[:, 1024:1088], rotary[s])

    def soften(s, found):
        visible = position <= lengths[s]
        found = jnp.where(visible, found * (192.0**-0.5), -1e30)
        high, low = halves(jnp.max(found, axis=1, keepdims=True))
        weight = jnp.where(visible, jnp.exp(found - (high + low)), 0.0)
        t_high, t_low = halves(jnp.sum(weight, axis=1, keepdims=True))
        stats = jnp.where(
            lane == 0,
            high,
            jnp.where(lane == 1, low, jnp.where(lane == 2, t_high, t_low)),
        )
        return weight.astype(BF16), stats

    def mix(s, weight, stats):
        found = plain(weight, latent[span * s : span * s + span])
        mix_own[s, :, 0:1024] = found[0:depth]
        mix_own[s, :, 1024:1152] = stats[0:depth]
        mix_send[s, :, :, 0:1024] = found[depth:].astype(BF16).reshape(RING - 1, depth, 1024)
        mix_send[s, :, :, 1024:1152] = stats[depth:].astype(BF16).reshape(RING - 1, depth, 128)
        for e in order:
            send(mix_send.at[s, e - 1], mix_recv.at[s, e - 1], MIX, MIX + s, at(z, ym(e)))

    found = {0: score(0)}
    for s in range(8):
        if s < 7:
            found[s + 1] = score(s + 1)
        mix(s, *soften(s, found.pop(s)))

    def combine(parts):
        tops = [p[:, 1024:1025] + p[:, 1025:1026] for p in parts]
        sums = [p[:, 1026:1027] + p[:, 1027:1028] for p in parts]
        top = functools.reduce(jnp.maximum, tops)
        factors = [jnp.exp(t - top) for t in tops]
        total = sum(f * v for f, v in zip(factors, sums))
        return top, total, sum(f * p[:, 0:1024] for f, p in zip(factors, parts))

    lane8k = lane[0:depth]
    for s in range(8):
        arrived(mix_recv.at[s], MIX + s)
        top, total, found = combine(
            [mix_own[s]] + [mix_recv[s, e].astype(F32) for e in range(RING - 1)]
        )
        mix2_send[s, :, 0:1024] = found
        mix2_send[s, :, 1024:1152] = jnp.where(
            lane8k == 0, top, jnp.where(lane8k == 2, total, 0.0)
        )
        for d in near_first:
            own, theirs = mix2_send.at[s, pl.ds(d, 1)], mix2_recv.at[d, pl.ds(s, 1)]
            send(own, theirs, MIX2, MIX2, at(zm(d), y))
        mix2_recv[0, s : s + 1] = mix2_send[s, 0:1]

    loads.pop("payload").wait()
    loads.pop("w_out").wait()
    arrived(mix2_recv.at[1:depth], MIX2)
    _, total, found = combine([mix2_recv[d] for d in range(depth)])
    attended = (found / total).astype(BF16)

    values = plain(attended, payload[...]).astype(BF16)
    projected = plain(values, w_out[...])
    first = lane8 < 64
    for i in range(depth // 2):
        for j in range(RING):
            a = 128 * (2 * i * RING + j)
            b = 128 * ((2 * i + 1) * RING + j)
            one, two = projected[:, a : a + 128], projected[:, b : b + 128]
            out_send[j, 0, i] = jnp.where(first, one, pltpu.roll(two, 64, 1)).astype(BF16)
            out_send[j, 1, i] = jnp.where(first, pltpu.roll(one, 64, 1), two).astype(BF16)
    for e, c in plane:
        core = (tp + c) % 2
        theirs = out_recv.at[2 * e + c]
        send(out_send.at[yp(e), core], theirs, OUT, OUT, at(z, yp(e), core))
    found = out_send[y, tp].astype(F32)
    arrived(out_recv.at[1 : 2 * RING], OUT)
    for k in range(1, 2 * RING):
        found = found + out_recv[k].astype(F32)
    out2_send[...] = found.astype(BF16)
    for d in near_first:
        send(out2_send.at[zp(d) // 2], out2_recv.at[d], OUT2, OUT2, at(zp(d), y))
    found = out2_send[z // 2].astype(F32)
    arrived(out2_recv.at[1:depth], OUT2)
    for d in range(1, depth):
        found = found + out2_recv[d].astype(F32)
    attention_out[...] = jnp.where(z % 2 == 0, found[:, 0:64], found[:, 64:128])

    for ref, phase in (
        (part_recv, PART),
        (mid_recv.at[1:depth], MID),
        (full.at[1 : 2 * RING], FULL),
        (queries.at[0, 1:depth], ASK_Z),
        (queries.at[1:RING], ASK_Y),
        (mix_send, MIX),
        (mix2_recv.at[1:depth], MIX2),
        (out_recv.at[1 : 2 * RING], OUT),
        (out2_recv.at[1:depth], OUT2),
    ):
        describe(ref, ref, phase, 0, at(z, y)).wait_send()


def settle(a, b, c, to_a, to_b, to_c):
    to_a[...] = a[...]
    to_b[...] = b[...]
    to_c[...] = c[...]


def local(
    depth,
    tokens,
    token_gain,
    asker_narrow_matrix,
    hidden_narrow_matrix,
    asker_multiplier,
    hidden_multiplier,
    asker_unspun_matrix,
    asker_spin_matrix,
    lock_widen_matrix,
    payload_widen_matrix,
    w_output,
    cache_latent,
    cache_rotary,
    lengths,
):
    operands = (
        tokens,
        token_gain.reshape(1, 128),
        asker_narrow_matrix,
        hidden_narrow_matrix.T,
        asker_multiplier.reshape(12, 128),
        hidden_multiplier.reshape(1, 1024),
        asker_unspun_matrix.reshape(1536, 128),
        asker_spin_matrix.reshape(1536, 64).T,
        lock_widen_matrix.reshape(128, 1024),
        payload_widen_matrix.reshape(1024, 128),
        w_output,
        cache_latent.reshape(2048, 1024),
        jnp.swapaxes(cache_rotary, 1, 2),
    )
    hbm = pl.BlockSpec(memory_space=pl.ANY)
    vmem = pl.BlockSpec(memory_space=pltpu.VMEM)
    dma = pltpu.SemaphoreType.DMA
    shapes = tuple(jax.ShapeDtypeStruct((8, w), F32) for w in (64, 1024, 64))
    found = pl.pallas_call(
        functools.partial(kernel, depth),
        out_shape=shapes,
        in_specs=[hbm] * (len(operands) + 1),
        out_specs=(vmem, vmem, vmem),
        scratch_shapes=[pltpu.VMEM(a.shape, a.dtype) for a in operands]
        + [
            pltpu.VMEM((RING, 2, 3, 8, 128), F32),
            pltpu.VMEM((RING - 1, 3, 8, 128), F32),
            pltpu.VMEM((depth, 3, 8, 128), F32),
            pltpu.VMEM((2 * RING, 3, 8, 128), F32),
            pltpu.VMEM((RING, depth, 8, 1152), BF16),
            pltpu.VMEM((8, RING, depth, 1152), BF16),
            pltpu.VMEM((8, depth, 1152), F32),
            pltpu.VMEM((8, RING - 1, depth, 1152), BF16),
            pltpu.VMEM((8, RING - 1, depth, 1152), BF16),
            pltpu.VMEM((8, depth, 1152), F32),
            pltpu.VMEM((depth, 8, 1152), F32),
            pltpu.VMEM((RING, 2, depth // 2, 8, 128), BF16),
            pltpu.VMEM((2 * RING, depth // 2, 8, 128), BF16),
            pltpu.VMEM((depth // 2, 8, 128), BF16),
            pltpu.VMEM((depth, 8, 128), BF16),
            dma((len(operands) + 1,)),
            dma((PHASES,)),
            dma((PHASES,)),
            pltpu.SMEM((8,), jnp.int32),
        ],
        compiler_params=pltpu.CompilerParams(collective_id=0, has_side_effects=True),
    )(*operands, lengths)
    return pl.pallas_call(
        settle, out_shape=shapes, in_specs=[vmem] * 3, out_specs=(vmem, vmem, vmem)
    )(*found)


def solution(mesh):
    return jax.shard_map(
        functools.partial(local, mesh.shape["kv"] // RING),
        mesh=mesh,
        in_specs=(
            P("dp", "kv"),
            P("kv"),
            P("kv", None),
            P("kv", None),
            P(),
            P(),
            P(None, ("kv", "tp"), None),
            P(None, ("kv", "tp"), None),
            P(("kv", "tp"), None, None),
            P(("kv", "tp"), None, None),
            P(("kv", "tp"), None),
            P("dp", "kv", None),
            P("dp", "kv", None),
            P("dp"),
        ),
        out_specs=(P("dp", ("kv", "tp")), P("dp", None), P("dp", None)),
        check_vma=False,
    )
```

```python
import functools

import jax
import jax.numpy as jnp
from jax import lax
from jax.experimental import pallas as pl
from jax.experimental.pallas import tpu as pltpu
from jax.sharding import PartitionSpec as P

MODEL_BREADTH = 4096
EPS = 1e-06
THETA = 10000.0
RING = 4
MESH = pl.DeviceIdType.MESH
PART, MID, FULL, ASK_Y, ASK_Z, MIX, MIX2, OUT, PHASES = 0, 1, 2, 3, 8, 16, 24, 25, 26
F32 = jnp.float32
BF16 = jnp.bfloat16


def across(a, b):
    return lax.dot_general(a, b, (((1,), (1,)), ((), ())), preferred_element_type=F32)


def plain(a, b):
    return jnp.dot(a, b, preferred_element_type=F32)


def kernel(
    depth,
    tokens_hbm,
    gain_hbm,
    ask_hbm,
    hid_hbm,
    ask_gain_hbm,
    hid_gain_hbm,
    unspun_hbm,
    spin_hbm,
    lock_hbm,
    payload_hbm,
    out_hbm,
    latent_hbm,
    rotary_hbm,
    lengths_hbm,
    attention_out,
    hidden_out,
    spun_out,
    tokens,
    gain,
    ask,
    hid,
    ask_gain,
    hid_gain,
    unspun,
    spin,
    lock,
    payload,
    w_out,
    latent,
    rotary,
    part_send,
    part_recv,
    mid_recv,
    full,
    queries,
    sorted_queries,
    mix_own,
    mix_send,
    mix_recv,
    mix2_send,
    mix2_recv,
    out_send,
    out_recv,
    local_sem,
    sent_sems,
    come_sems,
    greeted,
    lengths,
):
    kv = lax.axis_index("kv")
    tp = lax.axis_index("tp")
    z, y = kv // RING, kv % RING
    span = 256
    near_first = sorted(range(1, depth), key=lambda d: min(d, depth - d))
    order = (1, 3, 2)

    def at(zz, yy, cc=None):
        where = {"kv": zz * RING + yy}
        if cc is not None:
            where["tp"] = cc
        return where

    def zp(d):
        return (z + d) % depth

    def zm(d):
        return (z + depth - d) % depth

    def yp(d):
        return (y + d) % RING

    def ym(d):
        return (y + RING - d) % RING

    def describe(src, dst, phase, arrival, device):
        return pltpu.make_async_remote_copy(
            src_ref=src,
            dst_ref=dst,
            send_sem=sent_sems.at[phase],
            recv_sem=come_sems.at[arrival],
            device_id=device,
            device_id_type=MESH,
        )

    def send(src, dst, phase, arrival, device):
        describe(src, dst, phase, arrival, device).start()

    def arrived(ref, arrival):
        describe(ref, ref, 0, arrival, at(z, y)).wait_recv()

    plane = [(e, c) for e in (*order, 0) for c in range(2) if e or c]

    barrier = pltpu.get_barrier_semaphore()

    def greet(device):
        pl.semaphore_signal(barrier, inc=1, device_id=device, device_id_type=MESH)

    for e in order:
        greet(at(z, yp(e), 0))
    for d in near_first:
        greet(at(zp(d), y, 1))

    @pl.when(tp == 0)
    def _():
        greet(at(z, y, 1))

    @pl.when(tp == 1)
    def _():
        greet(at(z, y, 0))

    def tell(which):
        pl.semaphore_signal(
            greeted.at[which], inc=1, device_id=at(z, y, (tp + 1) % 2), device_id_type=MESH
        )

    def plane_is_here():
        @pl.when(tp == 0)
        def _():
            pl.semaphore_wait(barrier, 2 * RING - 1)
            tell(0)

        @pl.when(tp == 1)
        def _():
            pl.semaphore_wait(greeted.at[0], 1)

    def line_is_here():
        @pl.when(tp == 1)
        def _():
            pl.semaphore_wait(barrier, 2 * depth - 1)
            tell(1)

        @pl.when(tp == 0)
        def _():
            pl.semaphore_wait(greeted.at[1], 1)

    loads = {}

    def load(**pairs):
        for name, (src, dst) in pairs.items():
            loads[name] = pltpu.make_async_copy(src, dst, local_sem.at[len(started)])
            started.append(name)
            loads[name].start()

    started = []
    load(
        tokens=(tokens_hbm, tokens),
        gain=(gain_hbm, gain),
        ask=(ask_hbm, ask),
        hid=(hid_hbm, hid),
    )

    for name in ("tokens", "gain", "ask", "hid"):
        loads.pop(name).wait()
    load(
        lengths=(lengths_hbm, lengths),
        ask_gain=(ask_gain_hbm, ask_gain),
        hid_gain=(hid_gain_hbm, hid_gain),
        unspun=(unspun_hbm, unspun),
        spin=(spin_hbm, spin),
        lock=(lock_hbm, lock),
        rotary=(rotary_hbm, rotary),
        latent=(latent_hbm, latent),
        payload=(payload_hbm, payload),
        w_out=(out_hbm, w_out),
    )
    wide = tokens[...].astype(F32)
    squares = jnp.sum(wide * wide, axis=1, keepdims=True)
    scaled = (wide * gain[...]).astype(BF16)
    query_part = plain(scaled, ask[...])
    latent_part = across(scaled, hid[...])
    tiles = [query_part[:, 128 * t : 128 * t + 128] for t in range(12)]
    tiles += [latent_part[:, 128 * t : 128 * t + 128] for t in range(8)]
    tiles += [
        jnp.concatenate([latent_part[:, 1024:1088], jnp.broadcast_to(squares, (8, 64))], axis=1)
    ]
    tiles += [jnp.zeros((8, 128), F32)] * 3
    for t, tile in enumerate(tiles):
        part_send[t // 6, t // 3 % 2, t % 3] = tile

    plane_is_here()
    for e in order:
        send(part_send.at[yp(e), tp], part_recv.at[e - 1], PART, PART, at(z, yp(e)))

    loads.pop("lengths").wait()
    row8 = lax.broadcasted_iota(jnp.int32, (8, 128), 0)
    lane8 = lax.broadcasted_iota(jnp.int32, (8, 128), 1)
    length_rows = jnp.zeros((8, 128), jnp.int32)
    frequency = jnp.zeros((8, 128), F32)
    for s in range(8):
        length_rows = jnp.where(row8 == s, lengths[s], length_rows)
    for i in range(32):
        frequency = jnp.where(lane8 % 32 == i, float(THETA ** (-i / 32)), frequency)
    angles = length_rows.astype(F32) * frequency
    cosine = jnp.cos(angles)
    sine = jnp.where(lane8 % 64 < 32, -jnp.sin(angles), jnp.sin(angles))

    def spinning(v):
        twice = jnp.concatenate([v, v], axis=1)
        return twice * cosine + pltpu.roll(twice, 32, 1) * sine

    total = part_send[y, tp]
    arrived(part_recv, PART)
    for e in range(RING - 1):
        total = total + part_recv[e]
    mid_recv[pl.ds(z, 1)] = total[None]
    line_is_here()
    for d in near_first:
        send(mid_recv.at[z], mid_recv.at[z], MID, MID, at(zp(d), y))
    arrived(mid_recv.at[1:depth], MID)
    total = mid_recv[0]
    for j in range(1, depth):
        total = total + mid_recv[j]
    full[pl.ds(2 * y + tp, 1)] = total[None]
    mine = full.at[2 * y + tp]
    for e, c in plane:
        send(mine, mine, FULL, FULL, at(z, yp(e), (tp + c) % 2))
    for name in ("unspun", "spin", "lock", "ask_gain", "hid_gain"):
        loads.pop(name).wait()
    arrived(full.at[1 : 2 * RING], FULL)

    last = full[6, 2]
    row_scale = lax.rsqrt(last[:, 64:65] / MODEL_BREADTH + EPS)
    query_down = jnp.concatenate([full[t // 3, t % 3] for t in range(12)], axis=1) * row_scale
    mean_square = jnp.mean(query_down * query_down, axis=1, keepdims=True)
    ask_gains = jnp.concatenate([ask_gain[t : t + 1] for t in range(12)], axis=1)
    squeezed = (query_down * lax.rsqrt(mean_square + EPS) * ask_gains).astype(BF16)
    nope = plain(squeezed, unspun[...]).astype(BF16)
    turned = spinning(across(squeezed, spin[...])).astype(BF16)
    queries[0, 0, :, 1024:1152] = turned
    queries[0, 0, :, 0:1024] = plain(nope, lock[...]).astype(BF16)

    def to_plane(d):
        for e in order:
            send(queries.at[0, d], queries.at[e, d], ASK_Y, ASK_Y + e, at(z, yp(e)))

    for d in near_first:
        send(queries.at[0, 0], queries.at[0, d], ASK_Z, ASK_Z + d, at(zp(d), y))
    to_plane(0)

    hidden_down = jnp.concatenate([full[t // 3, t % 3] for t in range(12, 20)], axis=1) * row_scale
    mean_square = jnp.mean(hidden_down * hidden_down, axis=1, keepdims=True)
    incoming_hidden = hidden_down * lax.rsqrt(mean_square + EPS) * hid_gain[...]
    incoming_spun = spinning(last[:, 0:64] * row_scale)[:, 0:64]
    hidden_out[...] = incoming_hidden
    spun_out[...] = incoming_spun

    loads.pop("latent").wait()
    loads.pop("rotary").wait()
    eye = (
        lax.broadcasted_iota(jnp.int32, (64, 64), 0) == lax.broadcasted_iota(jnp.int32, (64, 64), 1)
    ).astype(BF16)
    spun_columns = across(eye, incoming_spun.astype(BF16))
    position_row = kv * span + lax.broadcasted_iota(jnp.int32, (64, span), 1)
    position_column = kv * span + lax.broadcasted_iota(jnp.int32, (span, 1024), 0)
    for s in range(8):
        rotary[s] = jnp.where(
            position_row == lengths[s], spun_columns[:, s : s + 1], rotary[s].astype(F32)
        ).astype(BF16)
        latent[span * s : span * s + span] = jnp.where(
            position_column == lengths[s],
            incoming_hidden[s : s + 1],
            latent[span * s : span * s + span].astype(F32),
        ).astype(BF16)
        if s < depth - 1:
            d = near_first[s]
            arrived(queries.at[0, d], ASK_Z + d)
            to_plane(d)

    group = 8 * depth
    come = lax.broadcasted_iota(jnp.int32, (group, group), 1)
    went = lax.broadcasted_iota(jnp.int32, (group, group), 0)
    shuffle = (come == went % depth * 8 + went // depth).astype(BF16)

    def sort_rows(e):
        found = plain(shuffle, queries[e].reshape(group, 1152)).astype(BF16)
        sorted_queries[:, e] = found.reshape(8, depth, 1152)

    sort_rows(0)
    for e in order:
        arrived(queries.at[e], ASK_Y + e)
        sort_rows(e)

    heads = RING * depth
    position = kv * span + lax.broadcasted_iota(jnp.int32, (heads, span), 1)
    lane = lax.broadcasted_iota(jnp.int32, (heads, 128), 1)

    def halves(value):
        high = value.astype(BF16).astype(F32)
        return high, (value - high).astype(BF16).astype(F32)

    def score(s):
        block = latent[span * s : span * s + span]
        asked = sorted_queries[s].reshape(heads, 1152)
        return across(asked[:, 0:1024], block) + plain(asked[:, 1024:1088], rotary[s])

    def soften(s, found):
        visible = position <= lengths[s]
        found = jnp.where(visible, found * (192.0**-0.5), -1e30)
        high, low = halves(jnp.max(found, axis=1, keepdims=True))
        weight = jnp.where(visible, jnp.exp(found - (high + low)), 0.0)
        t_high, t_low = halves(jnp.sum(weight, axis=1, keepdims=True))
        stats = jnp.where(
            lane == 0,
            high,
            jnp.where(lane == 1, low, jnp.where(lane == 2, t_high, t_low)),
        )
        return weight.astype(BF16), stats

    def mix(s, weight, stats):
        found = plain(weight, latent[span * s : span * s + span])
        mix_own[s, :, 0:1024] = found[0:depth]
        mix_own[s, :, 1024:1152] = stats[0:depth]
        mix_send[s, :, :, 0:1024] = found[depth:].astype(BF16).reshape(RING - 1, depth, 1024)
        mix_send[s, :, :, 1024:1152] = stats[depth:].astype(BF16).reshape(RING - 1, depth, 128)
        for e in order:
            send(mix_send.at[s, e - 1], mix_recv.at[s, e - 1], MIX, MIX + s, at(z, ym(e)))

    found = {0: score(0)}
    for s in range(8):
        if s < 7:
            found[s + 1] = score(s + 1)
        mix(s, *soften(s, found.pop(s)))

    def combine(parts):
        tops = [p[:, 1024:1025] + p[:, 1025:1026] for p in parts]
        sums = [p[:, 1026:1027] + p[:, 1027:1028] for p in parts]
        top = functools.reduce(jnp.maximum, tops)
        factors = [jnp.exp(t - top) for t in tops]
        total = sum(f * v for f, v in zip(factors, sums))
        return top, total, sum(f * p[:, 0:1024] for f, p in zip(factors, parts))

    lane8k = lane[0:depth]
    for s in range(8):
        arrived(mix_recv.at[s], MIX + s)
        top, total, found = combine(
            [mix_own[s]] + [mix_recv[s, e].astype(F32) for e in range(RING - 1)]
        )
        mix2_send[s, :, 0:1024] = found
        mix2_send[s, :, 1024:1152] = jnp.where(
            lane8k == 0, top, jnp.where(lane8k == 2, total, 0.0)
        )
        for d in near_first:
            own, theirs = mix2_send.at[s, pl.ds(d, 1)], mix2_recv.at[d, pl.ds(s, 1)]
            send(own, theirs, MIX2, MIX2, at(zm(d), y))
        mix2_recv[0, s : s + 1] = mix2_send[s, 0:1]

    loads.pop("payload").wait()
    loads.pop("w_out").wait()
    arrived(mix2_recv.at[1:depth], MIX2)
    _, total, found = combine([mix2_recv[d] for d in range(depth)])
    attended = (found / total).astype(BF16)

    values = plain(attended, payload[...]).astype(BF16)
    projected = plain(values, w_out[...])
    kept = (row8 < 4) == (lane8 < 64)
    for k in range(RING * depth):
        tile = projected[:, 128 * k : 128 * k + 128]
        tile = jnp.where(kept, tile, pltpu.roll(pltpu.roll(tile, 64, 1), 4, 0)).astype(BF16)
        out_send[k, 0] = tile[0:4]
        out_send[k, 1] = tile[4:8]
    slot = 0
    for d in (*near_first, 0):
        for e, c in (*plane, (0, 0)):
            if d or e or c:
                core = (tp + c) % 2
                chip = zp(d) * RING + yp(e)
                own, theirs = out_send.at[chip, core], out_recv.at[slot]
                send(own, theirs, OUT, OUT, at(zp(d), yp(e), core))
                slot += 1
    found = out_send[kv, tp].astype(F32)
    arrived(out_recv, OUT)
    for k in range(slot):
        found = found + out_recv[k].astype(F32)
    attention_out[0:4] = found[:, 0:64]
    attention_out[4:8] = found[:, 64:128]

    for ref, phase in (
        (part_recv, PART),
        (mid_recv.at[1:depth], MID),
        (full.at[1 : 2 * RING], FULL),
        (queries.at[0, 1:depth], ASK_Z),
        (queries.at[1:RING], ASK_Y),
        (mix_send, MIX),
        (mix2_recv.at[1:depth], MIX2),
        (out_recv, OUT),
    ):
        describe(ref, ref, phase, 0, at(z, y)).wait_send()


def settle(a, b, c, to_a, to_b, to_c):
    to_a[...] = a[...]
    to_b[...] = b[...]
    to_c[...] = c[...]


def local(
    depth,
    tokens,
    token_gain,
    asker_narrow_matrix,
    hidden_narrow_matrix,
    asker_multiplier,
    hidden_multiplier,
    asker_unspun_matrix,
    asker_spin_matrix,
    lock_widen_matrix,
    payload_widen_matrix,
    w_output,
    cache_latent,
    cache_rotary,
    lengths,
):
    operands = (
        tokens,
        token_gain.reshape(1, 128),
        asker_narrow_matrix,
        hidden_narrow_matrix.T,
        asker_multiplier.reshape(12, 128),
        hidden_multiplier.reshape(1, 1024),
        asker_unspun_matrix.reshape(1536, 128),
        asker_spin_matrix.reshape(1536, 64).T,
        lock_widen_matrix.reshape(128, 1024),
        payload_widen_matrix.reshape(1024, 128),
        w_output,
        cache_latent.reshape(2048, 1024),
        jnp.swapaxes(cache_rotary, 1, 2),
    )
    hbm = pl.BlockSpec(memory_space=pl.ANY)
    vmem = pl.BlockSpec(memory_space=pltpu.VMEM)
    dma = pltpu.SemaphoreType.DMA
    shapes = tuple(jax.ShapeDtypeStruct((8, w), F32) for w in (64, 1024, 64))
    found = pl.pallas_call(
        functools.partial(kernel, depth),
        out_shape=shapes,
        in_specs=[hbm] * (len(operands) + 1),
        out_specs=(vmem, vmem, vmem),
        scratch_shapes=[pltpu.VMEM(a.shape, a.dtype) for a in operands]
        + [
            pltpu.VMEM((RING, 2, 3, 8, 128), F32),
            pltpu.VMEM((RING - 1, 3, 8, 128), F32),
            pltpu.VMEM((depth, 3, 8, 128), F32),
            pltpu.VMEM((2 * RING, 3, 8, 128), F32),
            pltpu.VMEM((RING, depth, 8, 1152), BF16),
            pltpu.VMEM((8, RING, depth, 1152), BF16),
            pltpu.VMEM((8, depth, 1152), F32),
            pltpu.VMEM((8, RING - 1, depth, 1152), BF16),
            pltpu.VMEM((8, RING - 1, depth, 1152), BF16),
            pltpu.VMEM((8, depth, 1152), F32),
            pltpu.VMEM((depth, 8, 1152), F32),
            pltpu.VMEM((RING * depth, 2, 4, 128), BF16),
            pltpu.VMEM((2 * RING * depth - 1, 4, 128), BF16),
            dma((len(operands) + 1,)),
            dma((PHASES,)),
            dma((PHASES,)),
            pltpu.SemaphoreType.REGULAR((2,)),
            pltpu.SMEM((8,), jnp.int32),
        ],
        compiler_params=pltpu.CompilerParams(collective_id=0, has_side_effects=True),
    )(*operands, lengths)
    return pl.pallas_call(
        settle, out_shape=shapes, in_specs=[vmem] * 3, out_specs=(vmem, vmem, vmem)
    )(*found)


def solution(mesh):
    return jax.shard_map(
        functools.partial(local, mesh.shape["kv"] // RING),
        mesh=mesh,
        in_specs=(
            P("dp", "kv"),
            P("kv"),
            P("kv", None),
            P("kv", None),
            P(),
            P(),
            P(None, ("kv", "tp"), None),
            P(None, ("kv", "tp"), None),
            P(("kv", "tp"), None, None),
            P(("kv", "tp"), None, None),
            P(("kv", "tp"), None),
            P("dp", "kv", None),
            P("dp", "kv", None),
            P("dp"),
        ),
        out_specs=(P("dp", ("kv", "tp")), P("dp", None), P("dp", None)),
        check_vma=False,
    )
```

```python
import functools

import jax
import jax.numpy as jnp
from jax import lax
from jax.experimental import pallas as pl
from jax.experimental.pallas import tpu as pltpu
from jax.sharding import PartitionSpec as P

MODEL_BREADTH = 4096
EPS = 1e-06
THETA = 10000.0
RING = 4
MESH = pl.DeviceIdType.MESH
PART, MID, FULL, ASK_Y, ASK_Z, MIX, MIX2, OUT, ASK_X, PHASES = 0, 1, 2, 3, 11, 27, 35, 36, 37, 38
F32 = jnp.float32
BF16 = jnp.bfloat16


def across(a, b):
    return lax.dot_general(a, b, (((1,), (1,)), ((), ())), preferred_element_type=F32)


def plain(a, b):
    return jnp.dot(a, b, preferred_element_type=F32)


def kernel(
    depth,
    tokens_hbm,
    gain_hbm,
    ask_hbm,
    hid_hbm,
    ask_gain_hbm,
    hid_gain_hbm,
    unspun_hbm,
    spin_hbm,
    lock_hbm,
    payload_hbm,
    out_hbm,
    latent_hbm,
    rotary_hbm,
    lengths_hbm,
    attention_out,
    hidden_out,
    spun_out,
    tokens,
    gain,
    ask,
    hid,
    ask_gain,
    hid_gain,
    unspun,
    spin,
    lock,
    payload,
    w_out,
    latent,
    rotary,
    part_send,
    part_recv,
    mid_recv,
    full,
    queries,
    sorted_queries,
    mix_own,
    mix_send,
    mix_recv,
    mix2_send,
    mix2_recv,
    out_send,
    out_recv,
    local_sem,
    sent_sems,
    come_sems,
    greeted,
    lengths,
):
    kv = lax.axis_index("kv")
    tp = lax.axis_index("tp")
    z, y = kv // RING, kv % RING
    span = 256
    far_first = sorted(range(1, depth), key=lambda d: -min(d, depth - d))
    order = (2, 1, 3)

    def at(zz, yy, cc=None):
        where = {"kv": zz * RING + yy}
        if cc is not None:
            where["tp"] = cc
        return where

    def zp(d):
        return (z + d) % depth

    def zm(d):
        return (z + depth - d) % depth

    def yp(d):
        return (y + d) % RING

    def ym(d):
        return (y + RING - d) % RING

    def describe(src, dst, phase, arrival, device):
        return pltpu.make_async_remote_copy(
            src_ref=src,
            dst_ref=dst,
            send_sem=sent_sems.at[phase],
            recv_sem=come_sems.at[arrival],
            device_id=device,
            device_id_type=MESH,
        )

    def send(src, dst, phase, arrival, device):
        describe(src, dst, phase, arrival, device).start()

    def arrived(ref, arrival):
        describe(ref, ref, 0, arrival, at(z, y)).wait_recv()

    plane = [(e, c) for e in (*order, 0) for c in range(2) if e or c]

    barrier = pltpu.get_barrier_semaphore()

    def greet(device):
        pl.semaphore_signal(barrier, inc=1, device_id=device, device_id_type=MESH)

    for e in order:
        greet(at(z, yp(e), 0))
    for d in far_first:
        greet(at(zp(d), y, 1))

    @pl.when(tp == 0)
    def _():
        greet(at(z, y, 1))

    @pl.when(tp == 1)
    def _():
        greet(at(z, y, 0))

    def tell(which):
        pl.semaphore_signal(
            greeted.at[which], inc=1, device_id=at(z, y, (tp + 1) % 2), device_id_type=MESH
        )

    def plane_is_here():
        @pl.when(tp == 0)
        def _():
            pl.semaphore_wait(barrier, 2 * RING - 1)
            tell(0)

        @pl.when(tp == 1)
        def _():
            pl.semaphore_wait(greeted.at[0], 1)

    def line_is_here():
        @pl.when(tp == 1)
        def _():
            pl.semaphore_wait(barrier, 2 * depth - 1)
            tell(1)

        @pl.when(tp == 0)
        def _():
            pl.semaphore_wait(greeted.at[1], 1)

    loads = {}

    def load(**pairs):
        for name, (src, dst) in pairs.items():
            loads[name] = pltpu.make_async_copy(src, dst, local_sem.at[len(started)])
            started.append(name)
            loads[name].start()

    started = []
    load(
        tokens=(tokens_hbm, tokens),
        gain=(gain_hbm, gain),
        ask=(ask_hbm, ask),
        hid=(hid_hbm, hid),
    )

    for name in ("tokens", "gain", "ask", "hid"):
        loads.pop(name).wait()
    load(
        lengths=(lengths_hbm, lengths),
        ask_gain=(ask_gain_hbm, ask_gain),
        hid_gain=(hid_gain_hbm, hid_gain),
        unspun=(unspun_hbm, unspun),
        spin=(spin_hbm, spin),
        lock=(lock_hbm, lock),
        rotary=(rotary_hbm, rotary),
        latent=(latent_hbm, latent),
        payload=(payload_hbm, payload),
        w_out=(out_hbm, w_out),
    )
    wide = tokens[...].astype(F32)
    squares = jnp.sum(wide * wide, axis=1, keepdims=True)
    scaled = (wide * gain[...]).astype(BF16)
    query_part = plain(scaled, ask[...])
    latent_part = across(scaled, hid[...])
    tiles = [query_part[:, 128 * t : 128 * t + 128] for t in range(12)]
    tiles += [latent_part[:, 128 * t : 128 * t + 128] for t in range(8)]
    tiles += [
        jnp.concatenate([latent_part[:, 1024:1088], jnp.broadcast_to(squares, (8, 64))], axis=1)
    ]
    tiles += [jnp.zeros((8, 128), F32)] * 3
    for t, tile in enumerate(tiles):
        part_send[t // 6, t // 3 % 2, t % 3] = tile

    plane_is_here()
    for e in order:
        send(part_send.at[yp(e), tp], part_recv.at[e - 1], PART, PART, at(z, yp(e)))

    loads.pop("lengths").wait()
    row8 = lax.broadcasted_iota(jnp.int32, (8, 128), 0)
    lane8 = lax.broadcasted_iota(jnp.int32, (8, 128), 1)
    length_rows = jnp.zeros((8, 128), jnp.int32)
    frequency = jnp.zeros((8, 128), F32)
    for s in range(8):
        length_rows = jnp.where(row8 == s, lengths[s], length_rows)
    for i in range(32):
        frequency = jnp.where(lane8 % 32 == i, float(THETA ** (-i / 32)), frequency)
    angles = length_rows.astype(F32) * frequency
    cosine = jnp.cos(angles)
    sine = jnp.where(lane8 % 64 < 32, -jnp.sin(angles), jnp.sin(angles))

    def spinning(v):
        twice = jnp.concatenate([v, v], axis=1)
        return twice * cosine + pltpu.roll(twice, 32, 1) * sine

    total = part_send[y, tp]
    arrived(part_recv, PART)
    for e in range(RING - 1):
        total = total + part_recv[e]
    mid_recv[pl.ds(z, 1)] = total[None]
    line_is_here()
    for d in far_first:
        send(mid_recv.at[z], mid_recv.at[z], MID, MID, at(zp(d), y))
    arrived(mid_recv.at[1:depth], MID)
    total = mid_recv[0]
    for j in range(1, depth):
        total = total + mid_recv[j]
    full[pl.ds(2 * y + tp, 1)] = total[None]
    mine = full.at[2 * y + tp]
    for e, c in plane:
        send(mine, mine, FULL, FULL, at(z, yp(e), (tp + c) % 2))
    for name in ("unspun", "spin", "lock", "ask_gain", "hid_gain"):
        loads.pop(name).wait()
    arrived(full.at[1 : 2 * RING], FULL)

    last = full[6, 2]
    row_scale = lax.rsqrt(last[:, 64:65] / MODEL_BREADTH + EPS)
    query_down = jnp.concatenate([full[t // 3, t % 3] for t in range(12)], axis=1) * row_scale
    mean_square = jnp.mean(query_down * query_down, axis=1, keepdims=True)
    ask_gains = jnp.concatenate([ask_gain[t : t + 1] for t in range(12)], axis=1)
    squeezed = (query_down * lax.rsqrt(mean_square + EPS) * ask_gains).astype(BF16)
    nope = plain(squeezed, unspun[...]).astype(BF16)
    turned = spinning(across(squeezed, spin[...]))
    absorbed = plain(nope, lock[...])
    for h in range(2):
        queries[h, 0, 0, :, 1024:1152] = turned[4 * h : 4 * h + 4].astype(BF16)
        queries[h, 0, 0, :, 0:1024] = absorbed[4 * h : 4 * h + 4].astype(BF16)

    def to_plane(h, d):
        for e in order:
            if h and d and e == 2:
                continue
            come = ASK_X if h and e == 2 else ASK_Y + RING * h + e
            send(queries.at[h, 0, d], queries.at[h, e, d], ASK_Y, come, at(z, yp(e)))

    def to_line(h, e):
        for d in far_first:
            if e:
                come = ASK_Y + RING * h + e
            else:
                come = ASK_Z + depth * h + d
            send(queries.at[h, e, 0], queries.at[h, e, d], ASK_Z, come, at(zp(d), y))

    to_line(0, 0)
    to_plane(0, 0)
    to_plane(1, 0)
    to_line(1, 0)

    hidden_down = jnp.concatenate([full[t // 3, t % 3] for t in range(12, 20)], axis=1) * row_scale
    mean_square = jnp.mean(hidden_down * hidden_down, axis=1, keepdims=True)
    incoming_hidden = hidden_down * lax.rsqrt(mean_square + EPS) * hid_gain[...]
    incoming_spun = spinning(last[:, 0:64] * row_scale)[:, 0:64]
    hidden_out[...] = incoming_hidden
    spun_out[...] = incoming_spun

    loads.pop("latent").wait()
    loads.pop("rotary").wait()
    eye = (
        lax.broadcasted_iota(jnp.int32, (64, 64), 0) == lax.broadcasted_iota(jnp.int32, (64, 64), 1)
    ).astype(BF16)
    spun_columns = across(eye, incoming_spun.astype(BF16))
    position_row = kv * span + lax.broadcasted_iota(jnp.int32, (64, span), 1)
    position_column = kv * span + lax.broadcasted_iota(jnp.int32, (span, 1024), 0)

    def renew(s):
        rotary[s] = jnp.where(
            position_row == lengths[s], spun_columns[:, s : s + 1], rotary[s].astype(F32)
        ).astype(BF16)
        latent[span * s : span * s + span] = jnp.where(
            position_column == lengths[s],
            incoming_hidden[s : s + 1],
            latent[span * s : span * s + span].astype(F32),
        ).astype(BF16)

    stale = list(range(8))
    for h in range(2):
        for d in far_first:
            if stale:
                renew(stale.pop(0))
            arrived(queries.at[h, 0, d], ASK_Z + depth * h + d)
            to_plane(h, d)
            if h == 0 and d == far_first[4]:
                arrived(queries.at[1, 2, 0], ASK_X)
                to_line(1, 2)

    group = 4 * depth
    come = lax.broadcasted_iota(jnp.int32, (group, group), 1)
    went = lax.broadcasted_iota(jnp.int32, (group, group), 0)
    shuffle = (come == went % depth * 4 + went // depth).astype(BF16)

    def sort_rows(h, e):
        found = plain(shuffle, queries[h, e].reshape(group, 1152)).astype(BF16)
        sorted_queries[4 * h : 4 * h + 4, e] = found.reshape(4, depth, 1152)

    sort_rows(0, 0)
    sort_rows(1, 0)

    heads = RING * depth
    position = kv * span + lax.broadcasted_iota(jnp.int32, (heads, span), 1)
    lane = lax.broadcasted_iota(jnp.int32, (heads, 128), 1)

    def halves(value):
        high = value.astype(BF16).astype(F32)
        return high, (value - high).astype(BF16).astype(F32)

    def score(s):
        block = latent[span * s : span * s + span]
        asked = sorted_queries[s].reshape(heads, 1152)
        return across(asked[:, 0:1024], block) + plain(asked[:, 1024:1088], rotary[s])

    def soften(s, found):
        visible = position <= lengths[s]
        found = jnp.where(visible, found * (192.0**-0.5), -1e30)
        high, low = halves(jnp.max(found, axis=1, keepdims=True))
        weight = jnp.where(visible, jnp.exp(found - (high + low)), 0.0)
        t_high, t_low = halves(jnp.sum(weight, axis=1, keepdims=True))
        stats = jnp.where(
            lane == 0,
            high,
            jnp.where(lane == 1, low, jnp.where(lane == 2, t_high, t_low)),
        )
        return weight.astype(BF16), stats

    def mix(s, weight, stats):
        found = plain(weight, latent[span * s : span * s + span])
        mix_own[s, :, 0:1024] = found[0:depth]
        mix_own[s, :, 1024:1152] = stats[0:depth]
        mix_send[s, :, :, 0:1024] = found[depth:].astype(BF16).reshape(RING - 1, depth, 1024)
        mix_send[s, :, :, 1024:1152] = stats[depth:].astype(BF16).reshape(RING - 1, depth, 128)
        for e in order:
            send(mix_send.at[s, e - 1], mix_recv.at[s, e - 1], MIX, MIX + s, at(z, ym(e)))

    for h in range(2):
        for e in order:
            arrived(queries.at[h, e, int(h == 1 and e == 2) :], ASK_Y + RING * h + e)
            sort_rows(h, e)
        found = {4 * h: score(4 * h)}
        for s in range(4 * h, 4 * h + 4):
            if s < 4 * h + 3:
                found[s + 1] = score(s + 1)
            mix(s, *soften(s, found.pop(s)))

    def combine(parts):
        tops = [p[:, 1024:1025] + p[:, 1025:1026] for p in parts]
        sums = [p[:, 1026:1027] + p[:, 1027:1028] for p in parts]
        top = functools.reduce(jnp.maximum, tops)
        factors = [jnp.exp(t - top) for t in tops]
        total = sum(f * v for f, v in zip(factors, sums))
        return top, total, sum(f * p[:, 0:1024] for f, p in zip(factors, parts))

    lane8k = lane[0:depth]
    for s in range(8):
        arrived(mix_recv.at[s], MIX + s)
        top, total, found = combine(
            [mix_own[s]] + [mix_recv[s, e].astype(F32) for e in range(RING - 1)]
        )
        mix2_send[s, :, 0:1024] = found
        mix2_send[s, :, 1024:1152] = jnp.where(
            lane8k == 0, top, jnp.where(lane8k == 2, total, 0.0)
        )
        for d in far_first:
            own, theirs = mix2_send.at[s, pl.ds(d, 1)], mix2_recv.at[d, pl.ds(s, 1)]
            send(own, theirs, MIX2, MIX2, at(zm(d), y))
        mix2_recv[0, s : s + 1] = mix2_send[s, 0:1]

    loads.pop("payload").wait()
    loads.pop("w_out").wait()
    arrived(mix2_recv.at[1:depth], MIX2)
    _, total, found = combine([mix2_recv[d] for d in range(depth)])
    attended = (found / total).astype(BF16)

    values = plain(attended, payload[...]).astype(BF16)
    projected = plain(values, w_out[...])
    kept = (row8 < 4) == (lane8 < 64)
    for k in range(RING * depth):
        tile = projected[:, 128 * k : 128 * k + 128]
        tile = jnp.where(kept, tile, pltpu.roll(pltpu.roll(tile, 64, 1), 4, 0)).astype(BF16)
        out_send[k, 0] = tile[0:4]
        out_send[k, 1] = tile[4:8]
    slot = 0
    for d in (*far_first, 0):
        for e, c in (*plane, (0, 0)):
            if d or e or c:
                core = (tp + c) % 2
                chip = zp(d) * RING + yp(e)
                own, theirs = out_send.at[chip, core], out_recv.at[slot]
                send(own, theirs, OUT, OUT, at(zp(d), yp(e), core))
                slot += 1
    found = out_send[kv, tp].astype(F32)
    arrived(out_recv, OUT)
    for k in range(slot):
        found = found + out_recv[k].astype(F32)
    attention_out[0:4] = found[:, 0:64]
    attention_out[4:8] = found[:, 64:128]

    for ref, phase in (
        (part_recv, PART),
        (mid_recv.at[1:depth], MID),
        (full.at[1 : 2 * RING], FULL),
        (queries.at[:, 0, 1:depth], ASK_Z),
        (queries.at[1, 2, 1:depth], ASK_Z),
        (queries.at[0, 1:RING], ASK_Y),
        (queries.at[1, 0:2], ASK_Y),
        (queries.at[1, 0, 0], ASK_Y),
        (mix_send, MIX),
        (mix2_recv.at[1:depth], MIX2),
        (out_recv, OUT),
    ):
        describe(ref, ref, phase, 0, at(z, y)).wait_send()


def settle(a, b, c, to_a, to_b, to_c):
    to_a[...] = a[...]
    to_b[...] = b[...]
    to_c[...] = c[...]


def local(
    depth,
    tokens,
    token_gain,
    asker_narrow_matrix,
    hidden_narrow_matrix,
    asker_multiplier,
    hidden_multiplier,
    asker_unspun_matrix,
    asker_spin_matrix,
    lock_widen_matrix,
    payload_widen_matrix,
    w_output,
    cache_latent,
    cache_rotary,
    lengths,
):
    operands = (
        tokens,
        token_gain.reshape(1, 128),
        asker_narrow_matrix,
        hidden_narrow_matrix.T,
        asker_multiplier.reshape(12, 128),
        hidden_multiplier.reshape(1, 1024),
        asker_unspun_matrix.reshape(1536, 128),
        asker_spin_matrix.reshape(1536, 64).T,
        lock_widen_matrix.reshape(128, 1024),
        payload_widen_matrix.reshape(1024, 128),
        w_output,
        cache_latent.reshape(2048, 1024),
        jnp.swapaxes(cache_rotary, 1, 2),
    )
    hbm = pl.BlockSpec(memory_space=pl.ANY)
    vmem = pl.BlockSpec(memory_space=pltpu.VMEM)
    dma = pltpu.SemaphoreType.DMA
    shapes = tuple(jax.ShapeDtypeStruct((8, w), F32) for w in (64, 1024, 64))
    found = pl.pallas_call(
        functools.partial(kernel, depth),
        out_shape=shapes,
        in_specs=[hbm] * (len(operands) + 1),
        out_specs=(vmem, vmem, vmem),
        scratch_shapes=[pltpu.VMEM(a.shape, a.dtype) for a in operands]
        + [
            pltpu.VMEM((RING, 2, 3, 8, 128), F32),
            pltpu.VMEM((RING - 1, 3, 8, 128), F32),
            pltpu.VMEM((depth, 3, 8, 128), F32),
            pltpu.VMEM((2 * RING, 3, 8, 128), F32),
            pltpu.VMEM((2, RING, depth, 4, 1152), BF16),
            pltpu.VMEM((8, RING, depth, 1152), BF16),
            pltpu.VMEM((8, depth, 1152), F32),
            pltpu.VMEM((8, RING - 1, depth, 1152), BF16),
            pltpu.VMEM((8, RING - 1, depth, 1152), BF16),
            pltpu.VMEM((8, depth, 1152), F32),
            pltpu.VMEM((depth, 8, 1152), F32),
            pltpu.VMEM((RING * depth, 2, 4, 128), BF16),
            pltpu.VMEM((2 * RING * depth - 1, 4, 128), BF16),
            dma((len(operands) + 1,)),
            dma((PHASES,)),
            dma((PHASES,)),
            pltpu.SemaphoreType.REGULAR((2,)),
            pltpu.SMEM((8,), jnp.int32),
        ],
        compiler_params=pltpu.CompilerParams(collective_id=0, has_side_effects=True),
    )(*operands, lengths)
    return pl.pallas_call(
        settle, out_shape=shapes, in_specs=[vmem] * 3, out_specs=(vmem, vmem, vmem)
    )(*found)


def solution(mesh):
    return jax.shard_map(
        functools.partial(local, mesh.shape["kv"] // RING),
        mesh=mesh,
        in_specs=(
            P("dp", "kv"),
            P("kv"),
            P("kv", None),
            P("kv", None),
            P(),
            P(),
            P(None, ("kv", "tp"), None),
            P(None, ("kv", "tp"), None),
            P(("kv", "tp"), None, None),
            P(("kv", "tp"), None, None),
            P(("kv", "tp"), None),
            P("dp", "kv", None),
            P("dp", "kv", None),
            P("dp"),
        ),
        out_specs=(P("dp", ("kv", "tp")), P("dp", None), P("dp", None)),
        check_vma=False,
    )
```

```python
import functools

import jax
import jax.numpy as jnp
from jax import lax
from jax.experimental import pallas as pl
from jax.experimental.pallas import tpu as pltpu
from jax.sharding import PartitionSpec as P

MODEL_BREADTH = 4096
EPS = 1e-06
THETA = 10000.0
RING = 4
MESH = pl.DeviceIdType.MESH
PART, MID, FULL, ASK_Y, ASK_Z, MIX, MIX2, OUT, ASK_X, PHASES = 0, 1, 2, 3, 11, 27, 35, 36, 37, 38
SENT = (PART, MID, FULL, ASK_Y, ASK_Z, MIX, MIX2, OUT)
F32 = jnp.float32
BF16 = jnp.bfloat16


def across(a, b):
    return lax.dot_general(a, b, (((1,), (1,)), ((), ())), preferred_element_type=F32)


def plain(a, b):
    return jnp.dot(a, b, preferred_element_type=F32)


def kernel(
    depth,
    tokens_hbm,
    gain_hbm,
    ask_hbm,
    hid_hbm,
    ask_gain_hbm,
    hid_gain_hbm,
    unspun_hbm,
    spin_hbm,
    lock_hbm,
    payload_hbm,
    out_hbm,
    latent_hbm,
    rotary_hbm,
    lengths_hbm,
    attention_out,
    hidden_out,
    spun_out,
    tokens,
    gain,
    ask,
    hid,
    ask_gain,
    hid_gain,
    unspun,
    spin,
    lock,
    payload,
    w_out,
    latent,
    rotary,
    part_send,
    part_recv,
    mid_recv,
    full,
    queries,
    sorted_queries,
    mix_own,
    mix_send,
    mix_recv,
    mix2_send,
    mix2_recv,
    out_send,
    out_recv,
    local_sem,
    sent_sems,
    come_sems,
    greeted,
    lengths,
):
    kv = lax.axis_index("kv")
    tp = lax.axis_index("tp")
    z, y = kv // RING, kv % RING
    span = 256
    far_first = sorted(range(1, depth), key=lambda d: -min(d, depth - d))
    order = (2, 1, 3)

    def at(zz, yy, cc=None):
        where = {"kv": zz * RING + yy}
        if cc is not None:
            where["tp"] = cc
        return where

    def zp(d):
        return (z + d) % depth

    def zm(d):
        return (z + depth - d) % depth

    def yp(d):
        return (y + d) % RING

    def ym(d):
        return (y + RING - d) % RING

    def describe(src, dst, phase, arrival, device):
        return pltpu.make_async_remote_copy(
            src_ref=src,
            dst_ref=dst,
            send_sem=sent_sems.at[SENT.index(phase)],
            recv_sem=come_sems.at[arrival],
            device_id=device,
            device_id_type=MESH,
        )

    def send(src, dst, phase, arrival, device):
        describe(src, dst, phase, arrival, device).start()

    def arrived(ref, arrival):
        describe(ref, ref, 0, arrival, at(z, y)).wait_recv()

    plane = [(e, c) for e in (*order, 0) for c in range(2) if e or c]

    barrier = pltpu.get_barrier_semaphore()

    def greet(device):
        pl.semaphore_signal(barrier, inc=1, device_id=device, device_id_type=MESH)

    for e in order:
        greet(at(z, yp(e), 0))
    for d in far_first:
        greet(at(zp(d), y, 1))

    @pl.when(tp == 0)
    def _():
        greet(at(z, y, 1))

    @pl.when(tp == 1)
    def _():
        greet(at(z, y, 0))

    def tell(which):
        pl.semaphore_signal(
            greeted.at[which], inc=1, device_id=at(z, y, (tp + 1) % 2), device_id_type=MESH
        )

    def plane_is_here():
        @pl.when(tp == 0)
        def _():
            pl.semaphore_wait(barrier, 2 * RING - 1)
            tell(0)

        @pl.when(tp == 1)
        def _():
            pl.semaphore_wait(greeted.at[0], 1)

    def line_is_here():
        @pl.when(tp == 1)
        def _():
            pl.semaphore_wait(barrier, 2 * depth - 1)
            tell(1)

        @pl.when(tp == 0)
        def _():
            pl.semaphore_wait(greeted.at[1], 1)

    loads = {}

    def load(**pairs):
        for name, (src, dst) in pairs.items():
            loads[name] = pltpu.make_async_copy(src, dst, local_sem.at[len(started)])
            started.append(name)
            loads[name].start()

    started = []
    load(
        tokens=(tokens_hbm, tokens),
        gain=(gain_hbm, gain),
        ask=(ask_hbm, ask),
        hid=(hid_hbm, hid),
    )

    for name in ("tokens", "gain", "ask", "hid"):
        loads.pop(name).wait()
    load(
        lengths=(lengths_hbm, lengths),
        ask_gain=(ask_gain_hbm, ask_gain),
        hid_gain=(hid_gain_hbm, hid_gain),
        unspun=(unspun_hbm, unspun),
        spin=(spin_hbm, spin),
        lock=(lock_hbm, lock),
        rotary=(rotary_hbm, rotary),
        latent=(latent_hbm, latent),
        payload=(payload_hbm, payload),
        w_out=(out_hbm, w_out),
    )
    wide = tokens[...].astype(F32)
    squares = jnp.sum(wide * wide, axis=1, keepdims=True)
    scaled = (wide * gain[...]).astype(BF16)
    query_part = plain(scaled, ask[...])
    latent_part = across(scaled, hid[...])
    tiles = [query_part[:, 128 * t : 128 * t + 128] for t in range(12)]
    tiles += [latent_part[:, 128 * t : 128 * t + 128] for t in range(8)]
    tiles += [
        jnp.concatenate([latent_part[:, 1024:1088], jnp.broadcast_to(squares, (8, 64))], axis=1)
    ]
    tiles += [jnp.zeros((8, 128), F32)] * 3
    for t, tile in enumerate(tiles):
        part_send[t // 6, t // 3 % 2, t % 3] = tile

    plane_is_here()
    for e in order:
        send(part_send.at[yp(e), tp], part_recv.at[e - 1], PART, PART, at(z, yp(e)))

    loads.pop("lengths").wait()
    row8 = lax.broadcasted_iota(jnp.int32, (8, 128), 0)
    lane8 = lax.broadcasted_iota(jnp.int32, (8, 128), 1)
    length_rows = jnp.zeros((8, 128), jnp.int32)
    frequency = jnp.zeros((8, 128), F32)
    for s in range(8):
        length_rows = jnp.where(row8 == s, lengths[s], length_rows)
    for i in range(32):
        frequency = jnp.where(lane8 % 32 == i, float(THETA ** (-i / 32)), frequency)
    angles = length_rows.astype(F32) * frequency
    cosine = jnp.cos(angles)
    sine = jnp.where(lane8 % 64 < 32, -jnp.sin(angles), jnp.sin(angles))

    def spinning(v):
        twice = jnp.concatenate([v, v], axis=1)
        return twice * cosine + pltpu.roll(twice, 32, 1) * sine

    total = part_send[y, tp]
    arrived(part_recv, PART)
    for e in range(RING - 1):
        total = total + part_recv[e]
    mid_recv[pl.ds(z, 1)] = total[None]
    line_is_here()
    for d in far_first:
        send(mid_recv.at[z], mid_recv.at[z], MID, MID, at(zp(d), y))
    arrived(mid_recv.at[1:depth], MID)
    total = mid_recv[0]
    for j in range(1, depth):
        total = total + mid_recv[j]
    full[pl.ds(2 * y + tp, 1)] = total[None]
    mine = full.at[2 * y + tp]
    for e, c in plane:
        send(mine, mine, FULL, FULL, at(z, yp(e), (tp + c) % 2))
    for name in ("unspun", "spin", "lock", "ask_gain", "hid_gain"):
        loads.pop(name).wait()
    arrived(full.at[1 : 2 * RING], FULL)

    last = full[6, 2]
    row_scale = lax.rsqrt(last[:, 64:65] / MODEL_BREADTH + EPS)
    query_down = jnp.concatenate([full[t // 3, t % 3] for t in range(12)], axis=1) * row_scale
    mean_square = jnp.mean(query_down * query_down, axis=1, keepdims=True)
    ask_gains = jnp.concatenate([ask_gain[t : t + 1] for t in range(12)], axis=1)
    squeezed = (query_down * lax.rsqrt(mean_square + EPS) * ask_gains).astype(BF16)
    nope = plain(squeezed, unspun[...]).astype(BF16)
    turned = spinning(across(squeezed, spin[...]))
    absorbed = plain(nope, lock[...])
    for h in range(2):
        queries[h, 0, 0, :, 1024:1152] = turned[4 * h : 4 * h + 4].astype(BF16)
        queries[h, 0, 0, :, 0:1024] = absorbed[4 * h : 4 * h + 4].astype(BF16)

    def to_plane(h, d):
        for e in order:
            if h and d and e == 2:
                continue
            come = ASK_X if h and e == 2 else ASK_Y + RING * h + e
            send(queries.at[h, 0, d], queries.at[h, e, d], ASK_Y, come, at(z, yp(e)))

    def to_line(h, e):
        for d in far_first:
            if e:
                come = ASK_Y + RING * h + e
            else:
                come = ASK_Z + depth * h + d
            send(queries.at[h, e, 0], queries.at[h, e, d], ASK_Z, come, at(zp(d), y))

    to_line(0, 0)
    to_plane(0, 0)
    to_plane(1, 0)
    to_line(1, 0)

    hidden_down = jnp.concatenate([full[t // 3, t % 3] for t in range(12, 20)], axis=1) * row_scale
    mean_square = jnp.mean(hidden_down * hidden_down, axis=1, keepdims=True)
    incoming_hidden = hidden_down * lax.rsqrt(mean_square + EPS) * hid_gain[...]
    incoming_spun = spinning(last[:, 0:64] * row_scale)[:, 0:64]
    hidden_out[...] = incoming_hidden
    spun_out[...] = incoming_spun

    loads.pop("latent").wait()
    loads.pop("rotary").wait()
    eye = (
        lax.broadcasted_iota(jnp.int32, (64, 64), 0) == lax.broadcasted_iota(jnp.int32, (64, 64), 1)
    ).astype(BF16)
    spun_columns = across(eye, incoming_spun.astype(BF16))
    position_row = kv * span + lax.broadcasted_iota(jnp.int32, (64, span), 1)
    position_column = kv * span + lax.broadcasted_iota(jnp.int32, (span, 1024), 0)

    def renew(s):
        rotary[s] = jnp.where(
            position_row == lengths[s], spun_columns[:, s : s + 1], rotary[s].astype(F32)
        ).astype(BF16)
        latent[span * s : span * s + span] = jnp.where(
            position_column == lengths[s],
            incoming_hidden[s : s + 1],
            latent[span * s : span * s + span].astype(F32),
        ).astype(BF16)

    stale = list(range(8))
    for h in range(2):
        for d in far_first:
            if stale:
                renew(stale.pop(0))
            arrived(queries.at[h, 0, d], ASK_Z + depth * h + d)
            to_plane(h, d)
            if h == 0 and d == far_first[4]:
                arrived(queries.at[1, 2, 0], ASK_X)
                to_line(1, 2)

    group = 4 * depth
    come = lax.broadcasted_iota(jnp.int32, (group, group), 1)
    went = lax.broadcasted_iota(jnp.int32, (group, group), 0)
    shuffle = (come == went % depth * 4 + went // depth).astype(BF16)

    def sort_rows(h, e):
        found = plain(shuffle, queries[h, e].reshape(group, 1152)).astype(BF16)
        sorted_queries[4 * h : 4 * h + 4, e] = found.reshape(4, depth, 1152)

    sort_rows(0, 0)
    sort_rows(1, 0)

    heads = RING * depth
    position = kv * span + lax.broadcasted_iota(jnp.int32, (heads, span), 1)
    lane = lax.broadcasted_iota(jnp.int32, (heads, 128), 1)

    def halves(value):
        high = value.astype(BF16).astype(F32)
        return high, (value - high).astype(BF16).astype(F32)

    def score(s):
        block = latent[span * s : span * s + span]
        asked = sorted_queries[s].reshape(heads, 1152)
        return across(asked[:, 0:1024], block) + plain(asked[:, 1024:1088], rotary[s])

    def soften(s, found):
        visible = position <= lengths[s]
        found = jnp.where(visible, found * (192.0**-0.5), -1e30)
        high, low = halves(jnp.max(found, axis=1, keepdims=True))
        weight = jnp.where(visible, jnp.exp(found - (high + low)), 0.0)
        t_high, t_low = halves(jnp.sum(weight, axis=1, keepdims=True))
        stats = jnp.where(
            lane == 0,
            high,
            jnp.where(lane == 1, low, jnp.where(lane == 2, t_high, t_low)),
        )
        return weight.astype(BF16), stats

    def mix(s, weight, stats):
        found = plain(weight, latent[span * s : span * s + span])
        mix_own[s, :, 0:1024] = found[0:depth]
        mix_own[s, :, 1024:1152] = stats[0:depth]
        mix_send[s, :, :, 0:1024] = found[depth:].astype(BF16).reshape(RING - 1, depth, 1024)
        mix_send[s, :, :, 1024:1152] = stats[depth:].astype(BF16).reshape(RING - 1, depth, 128)
        for e in order:
            send(mix_send.at[s, e - 1], mix_recv.at[s, e - 1], MIX, MIX + s, at(z, ym(e)))

    for h in range(2):
        for e in order:
            arrived(queries.at[h, e, int(h == 1 and e == 2) :], ASK_Y + RING * h + e)
            sort_rows(h, e)
        found = {4 * h: score(4 * h)}
        for s in range(4 * h, 4 * h + 4):
            if s < 4 * h + 3:
                found[s + 1] = score(s + 1)
            mix(s, *soften(s, found.pop(s)))

    def combine(parts):
        tops = [p[:, 1024:1025] + p[:, 1025:1026] for p in parts]
        sums = [p[:, 1026:1027] + p[:, 1027:1028] for p in parts]
        top = functools.reduce(jnp.maximum, tops)
        factors = [jnp.exp(t - top) for t in tops]
        total = sum(f * v for f, v in zip(factors, sums))
        return top, total, sum(f * p[:, 0:1024] for f, p in zip(factors, parts))

    lane8k = lane[0:depth]
    for s in range(8):
        arrived(mix_recv.at[s], MIX + s)
        top, total, found = combine(
            [mix_own[s]] + [mix_recv[s, e].astype(F32) for e in range(RING - 1)]
        )
        mix2_send[s, :, 0:1024] = found
        mix2_send[s, :, 1024:1152] = jnp.where(
            lane8k == 0, top, jnp.where(lane8k == 2, total, 0.0)
        )
        for d in far_first:
            own, theirs = mix2_send.at[s, pl.ds(d, 1)], mix2_recv.at[d, pl.ds(s, 1)]
            send(own, theirs, MIX2, MIX2, at(zm(d), y))
        mix2_recv[0, s : s + 1] = mix2_send[s, 0:1]

    loads.pop("payload").wait()
    loads.pop("w_out").wait()
    arrived(mix2_recv.at[1:depth], MIX2)
    _, total, found = combine([mix2_recv[d] for d in range(depth)])
    attended = (found / total).astype(BF16)

    values = plain(attended, payload[...]).astype(BF16)
    projected = plain(values, w_out[...])
    kept = (row8 < 4) == (lane8 < 64)
    for k in range(RING * depth):
        tile = projected[:, 128 * k : 128 * k + 128]
        tile = jnp.where(kept, tile, pltpu.roll(pltpu.roll(tile, 64, 1), 4, 0)).astype(BF16)
        out_send[k, 0] = tile[0:4]
        out_send[k, 1] = tile[4:8]
    slot = 0
    for d in (*far_first, 0):
        for e, c in (*plane, (0, 0)):
            if d or e or c:
                core = (tp + c) % 2
                chip = zp(d) * RING + yp(e)
                own, theirs = out_send.at[chip, core], out_recv.at[slot]
                send(own, theirs, OUT, OUT, at(zp(d), yp(e), core))
                slot += 1
    found = out_send[kv, tp].astype(F32)
    arrived(out_recv, OUT)
    for k in range(slot):
        found = found + out_recv[k].astype(F32)
    attention_out[0:4] = found[:, 0:64]
    attention_out[4:8] = found[:, 64:128]

    for ref, phase in (
        (part_recv, PART),
        (mid_recv.at[1:depth], MID),
        (full.at[1 : 2 * RING], FULL),
        (queries.at[:, 0, 1:depth], ASK_Z),
        (queries.at[1, 2, 1:depth], ASK_Z),
        (queries.at[0, 1:RING], ASK_Y),
        (queries.at[1, 0:2], ASK_Y),
        (queries.at[1, 0, 0], ASK_Y),
        (mix_send, MIX),
        (mix2_recv.at[1:depth], MIX2),
        (out_recv, OUT),
    ):
        describe(ref, ref, phase, 0, at(z, y)).wait_send()


def settle(a, b, c, to_a, to_b, to_c):
    to_a[...] = a[...]
    to_b[...] = b[...]
    to_c[...] = c[...]


def local(
    depth,
    tokens,
    token_gain,
    asker_narrow_matrix,
    hidden_narrow_matrix,
    asker_multiplier,
    hidden_multiplier,
    asker_unspun_matrix,
    asker_spin_matrix,
    lock_widen_matrix,
    payload_widen_matrix,
    w_output,
    cache_latent,
    cache_rotary,
    lengths,
):
    operands = (
        tokens,
        token_gain.reshape(1, 128),
        asker_narrow_matrix,
        hidden_narrow_matrix.T,
        asker_multiplier.reshape(12, 128),
        hidden_multiplier.reshape(1, 1024),
        asker_unspun_matrix.reshape(1536, 128),
        asker_spin_matrix.reshape(1536, 64).T,
        lock_widen_matrix.reshape(128, 1024),
        payload_widen_matrix.reshape(1024, 128),
        w_output,
        cache_latent.reshape(2048, 1024),
        jnp.swapaxes(cache_rotary, 1, 2),
    )
    hbm = pl.BlockSpec(memory_space=pl.ANY)
    vmem = pl.BlockSpec(memory_space=pltpu.VMEM)
    dma = pltpu.SemaphoreType.DMA
    shapes = tuple(jax.ShapeDtypeStruct((8, w), F32) for w in (64, 1024, 64))
    found = pl.pallas_call(
        functools.partial(kernel, depth),
        out_shape=shapes,
        in_specs=[hbm] * (len(operands) + 1),
        out_specs=(vmem, vmem, vmem),
        scratch_shapes=[pltpu.VMEM(a.shape, a.dtype) for a in operands]
        + [
            pltpu.VMEM((RING, 2, 3, 8, 128), F32),
            pltpu.VMEM((RING - 1, 3, 8, 128), F32),
            pltpu.VMEM((depth, 3, 8, 128), F32),
            pltpu.VMEM((2 * RING, 3, 8, 128), F32),
            pltpu.VMEM((2, RING, depth, 4, 1152), BF16),
            pltpu.VMEM((8, RING, depth, 1152), BF16),
            pltpu.VMEM((8, depth, 1152), F32),
            pltpu.VMEM((8, RING - 1, depth, 1152), BF16),
            pltpu.VMEM((8, RING - 1, depth, 1152), BF16),
            pltpu.VMEM((8, depth, 1152), F32),
            pltpu.VMEM((depth, 8, 1152), F32),
            pltpu.VMEM((RING * depth, 2, 4, 128), BF16),
            pltpu.VMEM((2 * RING * depth - 1, 4, 128), BF16),
            dma((len(operands) + 1,)),
            dma((len(SENT),)),
            dma((PHASES,)),
            pltpu.SemaphoreType.REGULAR((2,)),
            pltpu.SMEM((8,), jnp.int32),
        ],
        compiler_params=pltpu.CompilerParams(collective_id=0, has_side_effects=True),
    )(*operands, lengths)
    return pl.pallas_call(
        settle, out_shape=shapes, in_specs=[vmem] * 3, out_specs=(vmem, vmem, vmem)
    )(*found)


def solution(mesh):
    return jax.shard_map(
        functools.partial(local, mesh.shape["kv"] // RING),
        mesh=mesh,
        in_specs=(
            P("dp", "kv"),
            P("kv"),
            P("kv", None),
            P("kv", None),
            P(),
            P(),
            P(None, ("kv", "tp"), None),
            P(None, ("kv", "tp"), None),
            P(("kv", "tp"), None, None),
            P(("kv", "tp"), None, None),
            P(("kv", "tp"), None),
            P("dp", "kv", None),
            P("dp", "kv", None),
            P("dp"),
        ),
        out_specs=(P("dp", ("kv", "tp")), P("dp", None), P("dp", None)),
        check_vma=False,
    )
```
